32 devices in a mesh: ep: 8 (over z, y), tp: 4 (over x, core).
Axes of the slice: x: 2, y: 2, z: 4, core: 2. Of those that a mesh axis runs over, the one named last changes fastest.
Arguments:
- outer_gate: bfloat16 [4096, 2048], P('ep', 'tp'), may hold values from -6 to 6
- inner_gate: bfloat16 [4096, 2048], P('ep', 'tp'), may hold values from -6 to 6
- conv_values: bfloat16 [4096, 2048], P('ep', 'tp'), may hold values from -6 to 6
- conv_taps: bfloat16 [3, 2048], P(None, 'tp'), may hold values from -3 to 3
- out_weight: bfloat16 [2048, 2048], P('tp'), may hold values from -0.125 to 0.125
- moe_input: bfloat16 [4096, 2048], P(('ep', 'tp')), may hold values from -6 to 6
- norm_gain: bfloat16 [2048], replicated, may hold values from 0.099609375 to 1.8984375
- gate_proj: bfloat16 [8, 2048, 1024], P('ep', None, 'tp'), may hold values from -0.125 to 0.125
- up_proj: bfloat16 [8, 2048, 1024], P('ep', None, 'tp'), may hold values from -0.125 to 0.125
- down_proj: bfloat16 [8, 1024, 2048], P('ep', 'tp'), may hold values from -0.1875 to 0.1875
- shared_gate: bfloat16 [2048, 1024], P(None, 'tp'), may hold values from -0.125 to 0.125
- shared_up: bfloat16 [2048, 1024], P(None, 'tp'), may hold values from -0.125 to 0.125
- shared_down: bfloat16 [1024, 2048], P('tp'), may hold values from -0.1875 to 0.1875
- routes: int32 [4096, 2], P('ep'), may hold values from 0 to 7, all different within a row; in each aligned block of 128 rows (0 to 127, 128 to 255, ...) at most 64 rows name the same one
- route_weight: float32 [4096, 2], P('ep'), may hold values from 0.3 to 1.5
Outputs:
- mixer_out: bfloat16 [4096, 2048], P(('ep', 'tp'))
- expert_mix: bfloat16 [4096, 2048], P(('ep', 'tp'))
The draws below stay inside these ranges and needn't reach their ends.
Inputs may be any that keep to these rules, and one draw needn't show every extreme that they name: `routes`: each row names 2 different experts. In the 128 rows of one device no expert is named more than 64 times, and in every draw some expert is named exactly 64 times in one device's rows.
All inputs are finite; a program needn't handle non-finite values.
Results may differ from the reference program's by a relative error of at most 0.012.
Values may be sent and summed in bfloat16 or wider, within the bound.
A program may use at most 128 MiB of HBM per device.

```python
import math
import jax
import jax.numpy as jnp
import numpy as np
from jax import lax

D = 2048
EH = 1024
SH = 1024
TOPK = 2
TAPS = 3
R2 = 128
EXPERTS = 8
CAP = 64
TOK1 = 4096
TOK2 = 4096
N_EP = 8
N_TP = 4


def block_scale(rng, dims, cuts, low, top_value):
    gain = 1.0
    for position, blocks in cuts:
        draws = jax.random.uniform(jax.random.fold_in(jax.random.fold_in(rng, 6), position), (blocks,), jnp.float32, low / len(cuts), top_value / len(cuts))
        gain = gain * jnp.repeat(jnp.exp(draws), dims[position] // blocks).reshape((-1,) + (1,) * (len(dims) - 1 - position))
    return gain


def assign_block(key, own, number, rows, number_of, top, limit, skew):
    ranking = jax.random.permutation(key, number_of)
    heavy_load, common = shares(number_of, rows * top, limit, skew, True), shares(number_of, rows * top, limit, skew, False)
    places = jnp.arange(number_of)

    def named(tallies, turn):
        used = int((tallies > 0).sum())
        fixed = max(1, used // 4)
        passed = fixed + (places - fixed + turn * (used - fixed)) % max(1, number_of - fixed)
        return jnp.zeros((number_of,), jnp.int32).at[ranking[jnp.where(places < fixed, places, passed)]].set(jnp.asarray(tallies, jnp.int32))

    tallies = jnp.where(number % 4 == 0, named(heavy_load, number // 4), named(common, number - number // 4 - 1))
    mixed = jax.random.permutation(jax.random.fold_in(own, 3), number_of)
    donor, receiver = mixed[0:number_of // 2 * 2:2], mixed[1:number_of // 2 * 2:2]
    room = jnp.minimum(tallies[donor] - 1, limit - tallies[receiver]) // 2
    room = jnp.where((donor == ranking[0]) | (receiver == ranking[0]) | (tallies[receiver] == 0), 0, jnp.maximum(room, 0))
    passed = jax.random.randint(jax.random.fold_in(own, 4), (number_of // 2,), 0, 1 << 20) % (room + 1)
    tallies = tallies.at[donor].add(-passed).at[receiver].add(passed)
    items = jnp.searchsorted(jnp.cumsum(tallies), jnp.arange(rows * top), side="right").astype(jnp.int32)
    table = items.reshape(top, rows).T
    table = table[jax.random.permutation(jax.random.fold_in(own, 1), rows)]
    turn = jax.random.randint(jax.random.fold_in(own, 2), (rows, 1), 0, top)
    return jnp.take_along_axis(table, (jnp.arange(top)[None, :] + turn) % top, axis=1)


def shares(count, total, bound, slope, full):
    weights = [(1 << 20) // math.isqrt(standing ** slope) + 1 for standing in range(1, count + 1)]
    largest = bound if full else min(bound, max(-(-total // count), total * weights[0] // sum(weights)))
    least = 1 if total - largest >= count - 1 else 0
    given, surplus = [largest] + [least] * (count - 1), total - largest - least * (count - 1)
    while surplus > 0:
        movable = [i for i in range(1, count) if given[i] < largest] or [i for i in range(1, count) if given[i] < bound]
        pool, budget = sum([weights[i] for i in movable]), surplus
        for i in movable:
            extra = min(bound - given[i], max(1, budget * weights[i] // pool), surplus)
            given[i] = given[i] + extra
            surplus = surplus - extra
    return np.array(given)


def normal_values(key, shape, spread, bound, split=(), held_as=jnp.bfloat16):
    drawn = jax.random.normal(key, shape, jnp.float32) * spread
    if len(split) > 0:
        drawn = block_scale(key, shape, split, -0.22, 0.18) * drawn
    return jnp.clip(drawn, min=-bound, max=bound).astype(held_as)


def setup_inputs(seed: int = 0) -> dict:
    key_of = jax.random.split(jax.random.key(seed), 16)
    outer_gate = normal_values(key_of[0], (TOK1, D), 1.0, 6.0, ((0, 8), (1, 4)))
    inner_gate = normal_values(key_of[1], (TOK1, D), 1.0, 6.0, ((0, 8), (1, 4)))
    conv_values = normal_values(key_of[2], (TOK1, D), 1.0, 6.0, ((0, 8), (1, 4)))
    conv_taps = normal_values(key_of[3], (TAPS, D), 0.577, 3.0, ((1, 4),))
    out_weight = normal_values(key_of[4], (D, D), D ** -0.5, 0.125, ((0, 4),))
    moe_input = normal_values(key_of[5], (TOK2, D), 1.0, 6.0, ((0, 32),))
    norm_gain = jnp.clip(1.0 + 0.18 * jax.random.normal(key_of[6], (D,), jnp.float32), 0.099609375, 1.8984375).astype(jnp.bfloat16)
    gate_proj = normal_values(key_of[7], (EXPERTS, D, EH), D ** -0.5, 0.125, ((0, 8), (2, 4)))
    up_proj = normal_values(key_of[8], (EXPERTS, D, EH), D ** -0.5, 0.125, ((0, 8), (2, 4)))
    down_proj = normal_values(key_of[9], (EXPERTS, EH, D), EH ** -0.5, 0.1875, ((0, 8), (1, 4)))
    shared_gate = normal_values(key_of[10], (D, SH), D ** -0.5, 0.125, ((1, 4),))
    shared_up = normal_values(key_of[11], (D, SH), D ** -0.5, 0.125, ((1, 4),))
    shared_down = normal_values(key_of[12], (SH, D), SH ** -0.5, 0.1875, ((0, 4),))
    routes_keys = jax.random.split(jax.random.fold_in(key_of[13], 1), TOK2 // R2)
    routes_turns = jax.random.permutation(jax.random.fold_in(key_of[13], 3), TOK2 // R2)
    routes = jax.vmap(lambda own, number: assign_block(jax.random.fold_in(key_of[13], 2), own, number, R2, N_EP, TOPK, CAP, 2))(routes_keys, routes_turns).reshape((TOK2, TOPK))
    route_weight = jnp.clip(0.3 + 1.2 * jax.random.uniform(key_of[14], (TOK2, TOPK), jnp.float32) ** block_scale(key_of[14], (TOK2, TOPK), ((0, 8),), -0.2, 0.2), 0.3, 1.5)
    return dict(outer_gate=outer_gate, inner_gate=inner_gate, conv_values=conv_values, conv_taps=conv_taps, out_weight=out_weight, moe_input=moe_input, norm_gain=norm_gain, gate_proj=gate_proj, up_proj=up_proj, down_proj=down_proj, shared_gate=shared_gate, shared_up=shared_up, shared_down=shared_down, routes=routes, route_weight=route_weight)


epsilon = 1e-06

def rms_norm(inputs, scales):
    values = inputs.astype(jnp.float32)
    square = lax.optimization_barrier(jnp.mean(values * values, axis=-1, keepdims=True))
    return (values * lax.rsqrt(square + epsilon) * scales.astype(jnp.float32)).astype(jnp.bfloat16)

def summed_parts(hidden, weight, pieces):
    stride = hidden.shape[1] // pieces
    result = jnp.zeros((hidden.shape[0], weight.shape[1]), jnp.float32)
    for piece_idx in range(pieces):
        partial_sum = jnp.dot(hidden[:, piece_idx * stride:(piece_idx + 1) * stride], weight[piece_idx * stride:(piece_idx + 1) * stride], preferred_element_type=jnp.float32).astype(jnp.bfloat16)
        partial_sum = lax.optimization_barrier(partial_sum)
        result = result + partial_sum.astype(jnp.float32)
    return result

def swiglu(inputs, gate_w, up_w):
    gate_term = jnp.dot(inputs, gate_w, preferred_element_type=jnp.float32)
    upward = jnp.dot(inputs, up_w, preferred_element_type=jnp.float32)
    return (jax.nn.silu(gate_term) * upward).astype(jnp.bfloat16)

def reference(outer_gate, inner_gate, conv_values, conv_taps, out_weight, moe_input, norm_gain, gate_proj, up_proj, down_proj, shared_gate, shared_up, shared_down, routes, route_weight):
    product = inner_gate.astype(jnp.float32) * conv_values.astype(jnp.float32)
    length = product.shape[0]
    padded = jnp.pad(product, ((TAPS - 1, 0), (0, 0)))
    tap_values = conv_taps.astype(jnp.float32)
    convolved = jnp.zeros_like(product)
    for offset in range(TAPS):
        convolved = convolved + tap_values[offset] * padded[offset:offset + length]
    gate_rows = (outer_gate.astype(jnp.float32) * convolved).astype(jnp.bfloat16)
    mixer_out = summed_parts(gate_rows, out_weight, N_TP).astype(jnp.bfloat16)
    normed = rms_norm(moe_input, norm_gain)
    tokens = normed.shape[0]
    slot_limit = N_EP * N_TP * CAP
    token_ids = jnp.arange(tokens, dtype=jnp.int32)

    def one_expert(running, operands):
        expert, gate_w, up_w, down_w = operands
        expert_hits = routes == expert
        chosen = jnp.any(expert_hits, axis=1)
        weight_sum = lax.optimization_barrier(jnp.sum(jnp.where(expert_hits, route_weight, jnp.float32(0.0)), axis=1))
        places = jnp.cumsum(chosen.astype(jnp.int32)) - 1
        targets = jnp.where(chosen, places, slot_limit).astype(jnp.int32)
        row_table = jnp.zeros((slot_limit,), jnp.int32).at[targets].set(token_ids, mode='drop')
        filled = jnp.zeros((slot_limit,), jnp.float32).at[targets].set(1.0, mode='drop')
        hidden = swiglu(normed[row_table], gate_w, up_w)
        result = summed_parts(hidden, down_w, N_TP).astype(jnp.bfloat16)
        result = lax.optimization_barrier(result)
        scaled = result.astype(jnp.float32) * (weight_sum[row_table] * filled)[:, None]
        return (running.at[row_table].add(scaled), None)
    routed, _ = lax.scan(one_expert, jnp.zeros((tokens, normed.shape[1]), jnp.float32), (jnp.arange(N_EP, dtype=jnp.int32), gate_proj, up_proj, down_proj))
    shared_hidden = swiglu(normed, shared_gate, shared_up)
    shared_sum = summed_parts(shared_hidden, shared_down, N_TP)
    expert_mix = (shared_sum + routed).astype(jnp.bfloat16)
    return (mixer_out, expert_mix)
```

```python
import functools

import jax
import jax.numpy as jnp
from jax import lax
from jax.experimental import pallas as pl
from jax.experimental.pallas import tpu as pltpu
from jax.sharding import PartitionSpec as P

epsilon = 1e-06
MESH = pl.DeviceIdType.MESH
f32 = jnp.float32
bf16 = jnp.bfloat16
CHUNKS = 4
MERGED = 3
NORMED_AT = 2


def dot(a, b):
    return jnp.dot(a, b, preferred_element_type=f32)


def kernel(
    dims,
    outer, inner, values, taps, out_w, tokens, gain, gate_p, up_p, down_p,
    sh_gate, sh_up, sh_down, routes, weights,
    mix_o, exp_o,
    l_tokens, l_gain, l_taps, l_routes, l_weights,
    l_outer, l_inner, l_values, halo, prod, l_out_w, l_sg, l_su, l_sd,
    gf, uf, df, nf, og, ld, hid, rt, rv,
    acc, parts, pairs, sums, arrived,
    loc_sem, halo_send, halo_recv, x_send, p_send, t_recv,
    d_send, d_recv, b_send, b_recv, r_send, r_recv, rx_send, rx_recv,
    ready_up, ready_down,
    g_routes, g_weights, g_blocks, g_rows, g_in, own_mix, gate_mix,
    gr_send, gr_recv, hb_send, hb_recv, g_send, g_recv, m_send, m_recv,
):
    ep, tp, cap = dims
    half = tp // 2
    e, t = lax.axis_index("ep"), lax.axis_index("tp")
    a, b = t // 2, lax.rem(t, 2)
    pair = (e, 2 * a + 1 - b)
    group, ch = l_inner.shape
    rows, width = tokens.shape
    slots = ep * cap
    cols = width // CHUNKS
    n_taps = taps.shape[0]

    def far(d):
        return 2 * lax.rem(a + d, half) + b

    def near(d):
        return 2 * lax.rem(a + half - d, half) + b

    def remote(src, dst, s, r, dev):
        return pltpu.make_async_remote_copy(
            src_ref=src, dst_ref=dst, send_sem=s, recv_sem=r, device_id=dev, device_id_type=MESH
        )

    barrier = pltpu.get_barrier_semaphore()

    def signal(sem, dev):
        pl.semaphore_signal(sem, inc=1, device_id=dev, device_id_type=MESH)

    levels = ep // 2
    level = e // 2
    below, above = level > 0, level < levels - 1
    lower, upper_dev = (jnp.maximum(e - 2, 0), t), (jnp.minimum(e + 2, ep - 1), t)
    signal(barrier, pair)
    for d in range(1, half):
        signal(barrier, (e, far(d)))
    chain = levels <= 4
    if chain:
        signal(barrier, (e + 1 - 2 * lax.rem(e, 2), t))

        @pl.when(below)
        def _():
            signal(barrier, lower)

        @pl.when(above)
        def _():
            signal(barrier, upper_dev)
    else:

        def greet(d, _):
            signal(barrier, (lax.rem(e + d, ep), t))
            return 0

        lax.fori_loop(1, ep, greet, 0)

    def ready_step(k):
        if not chain:
            return

        @pl.when(above)
        def _():
            signal(ready_up.at[k], upper_dev)

        @pl.when(below)
        def _():
            signal(ready_down.at[k], lower)

        @pl.when(below)
        def _():
            pl.semaphore_wait(ready_up.at[k], 1)

        @pl.when(above)
        def _():
            pl.semaphore_wait(ready_down.at[k], 1)

    small = [
        pltpu.make_async_copy(s, d, loc_sem.at[10 + i])
        for i, (s, d) in enumerate(
            (
                (tokens, l_tokens), (gain, l_gain), (routes, l_routes), (weights, l_weights),
                (taps, l_taps),
            )
        )
    ]
    for c in small:
        c.start()
    local = [
        pltpu.make_async_copy(s, d, loc_sem.at[i])
        for i, (s, d) in enumerate(
            (
                (inner, l_inner), (values, l_values), (outer, l_outer), (out_w, l_out_w),
                (sh_gate, l_sg), (sh_up, l_su), (sh_down, l_sd),
                (gate_p.at[0], gf.at[t]), (up_p.at[0], uf.at[t]), (down_p.at[0], df.at[t]),
            )
        )
    ]
    for c in local:
        c.start()

    if chain:
        pl.semaphore_wait(barrier, half + 1 + below.astype(jnp.int32) + above.astype(jnp.int32))
    else:
        pl.semaphore_wait(barrier, half + ep - 1)

    kinds = CHUNKS + 3
    n_kind = kinds - 1

    def land(k, s):
        if k == 0:
            return gf.at[s]
        if k == 1:
            return uf.at[s]
        if k == n_kind:
            return nf.at[s]
        return df.at[s, :, pl.ds((k - 2) * cols, cols)]

    def origin(k):
        if k == 0:
            return gate_p.at[0]
        if k == 1:
            return up_p.at[0]
        if k == n_kind:
            return nf.at[t]
        return down_p.at[0, :, pl.ds((k - 2) * cols, cols)]

    def x_copy(k, d):
        return remote(origin(k), land(k, t), x_send.at[k, d], t_recv.at[k, d], (e, far(d)))

    def pair_copy(k):
        return remote(origin(k), land(k, t), p_send.at[k, 0], t_recv.at[k, 0], pair)

    def forward_copy(k, d):
        s = near(d)
        return remote(land(k, s), land(k, s), p_send.at[k, d], t_recv.at[k, half - 1 + d], pair)

    def start_x(k):
        for d in range(1, half):
            x_copy(k, d).start()

    def forward(k):
        for d in range(1, half):
            x_copy(k, d).wait_recv()
            forward_copy(k, d).start()

    def wait_forwarded(k):
        for d in range(1, half):
            forward_copy(k, d).wait_recv()

    for k in range(3 + NORMED_AT):
        start_x(k)
    ready_step(0)
    for c in small:
        c.wait()
    mine = pl.ds(pl.multiple_of(t * rows, rows), rows)
    own_routes, own_w = l_routes[:, mine], l_weights[:, mine]

    def table(named, first, count):
        slot = lax.broadcasted_iota(jnp.int32, (count * cap, rows), 0)
        index = slot // cap
        place = (slot - index * cap).astype(f32)
        expert = index + first
        hit = jnp.zeros((count * cap, rows), f32)
        for k in range(named.shape[0]):
            hit = jnp.where(named[k : k + 1, :] == expert, 1.0, hit)
        upper = lax.broadcasted_iota(jnp.int32, (rows, rows), 0) < lax.broadcasted_iota(
            jnp.int32, (rows, rows), 1
        )
        earlier = dot(hit.astype(bf16), jnp.where(upper, 1.0, 0.0).astype(bf16))
        return jnp.where(earlier == place, hit, 0.0), expert

    def weighted(chosen, expert, named, given):
        scale = jnp.zeros(chosen.shape, f32)
        for k in range(named.shape[0]):
            scale = jnp.where(named[k : k + 1, :] == expert, given[k : k + 1, :], scale)
        full = jnp.transpose(chosen * scale)
        high = full.astype(bf16)
        return high, (full - high.astype(f32)).astype(bf16)

    chosen, expert = table(own_routes, 0, ep)
    sender = chosen.astype(bf16)

    if levels > 2:
        ready_step(1)
    scales = l_gain[...].astype(f32).reshape(1, width)

    def norm_rows(i, _):
        at = pl.ds(pl.multiple_of(i * 16, 16), 16)
        v = l_tokens[at, :].astype(f32)
        square = jnp.mean(v * v, axis=-1, keepdims=True)
        nf[t, at, :] = (v * lax.rsqrt(square + epsilon) * scales).astype(bf16)
        return 0

    lax.fori_loop(0, rows // 16, norm_rows, 0)

    for k in range(2, levels - 1):
        ready_step(k)

    def block(i):
        return pl.ds(pl.multiple_of(i * cap, cap), cap)

    def dispatch_copy(c, d):
        to = lax.rem(e + d, ep)
        at = pl.ds(c * cols, cols)
        return remote(
            og.at[block(to), at], ld.at[block(e), at], d_send.at[c, d], d_recv.at[c, d], (to, t)
        )

    for c in range(CHUNKS):
        at = pl.ds(c * cols, cols)
        og[:, at] = dot(sender, nf[t, :, at]).astype(bf16)

        def start_dispatch(d, _):
            dispatch_copy(c, d).start()
            return 0

        lax.fori_loop(1, ep, start_dispatch, 0)
        ld[block(e), at] = og[block(e), at]
    start_x(n_kind)
    for k in range(kinds):
        pair_copy(k).start()
    for k in range(3 + NORMED_AT, n_kind):
        start_x(k)
    here = e // 4
    place4 = lax.rem(e, 4)
    line = lax.rem(e, 2)
    inner_level = lax.rem(level, 2)
    is_gate = level == 1 + here
    other_gate = (jnp.minimum(2 * (2 - here) + line, ep - 1), t)

    def table_copies(i):
        return [
            remote(src.at[:, mine], dst.at[i], gr_send.at[n], gr_recv.at[n, i], other_gate)
            for n, (src, dst) in enumerate(((l_routes, g_routes), (l_weights, g_weights)))
        ]

    if chain:
        for c in table_copies(inner_level):
            c.start()
    edge = pl.ds(group - 16, 16)
    halos = [
        remote(src.at[edge, :], halo.at[i], halo_send.at[i], halo_recv.at[i], (lax.rem(e + 1, ep), t))
        for i, src in enumerate((inner, values))
    ]
    for c in halos:
        c.start()


    def pair_sum(j, i):
        return remote(
            parts.at[j, 2 * i + 1 - b], pairs.at[j, i], r_send.at[j, i], r_recv.at[j, i], pair
        )

    def far_sum(j, d, c):
        at = pl.ds(c * cols, cols)
        return remote(
            sums.at[j, d - 1, :, at], arrived.at[j, d - 1, :, at],
            rx_send.at[j, d, c], rx_recv.at[j, d, c], (e, far(d)),
        )

    def start_far(j):
        for d in range(1, half):
            i = lax.rem(a + d, half)
            pair_sum(j, i).wait_recv()
            for c in range(CHUNKS):
                at = pl.ds(c * cols, cols)
                total = parts[j, 2 * i + b, :, at].astype(f32) + pairs[j, i, :, at].astype(f32)
                sums[j, d - 1, :, at] = total.astype(bf16)
                far_sum(j, d, c).start()

    def summed(j, c):
        at = pl.ds(c * cols, cols)
        for d in range(1, half):
            far_sum(j, d, c).wait_recv()
        total = parts[j, t, :, at].astype(f32) + pairs[j, a, :, at].astype(f32)
        for d in range(1, half):
            total = total + arrived[j, d - 1, :, at].astype(f32)
        return total

    for c in local[:4]:
        c.wait()
    for c in halos:
        c.wait_recv()
    before = halo[0].astype(f32) * halo[1].astype(f32)
    prod[0:16, :] = jnp.where(e > 0, before, 0.0)
    prod[16:, :] = l_inner[...].astype(f32) * l_values[...].astype(f32)
    tap = l_taps[...].astype(f32)
    for s in range(tp):
        lo = s * rows
        conv = jnp.zeros((rows, ch), f32)
        for j in range(n_taps):
            first = 16 + lo - (n_taps - 1) + j
            conv = conv + tap[j : j + 1, :] * prod[first : first + rows, :]
        gated = (l_outer[lo : lo + rows, :].astype(f32) * conv).astype(bf16)
        for c in range(CHUNKS):
            at = pl.ds(c * cols, cols)
            parts[0, s, :, at] = dot(gated, l_out_w[:, at]).astype(bf16)
    for i in range(half):
        pair_sum(0, i).start()

    for c in local[4:]:
        c.wait()

    def shared(s):
        x = nf[s]
        g = dot(x, l_sg[...])
        u = dot(x, l_su[...])
        h = (g / (1.0 + jnp.exp(-g)) * u).astype(bf16)
        for c in range(CHUNKS):
            at = pl.ds(c * cols, cols)
            parts[1, s, :, at] = dot(h, l_sd[:, at]).astype(bf16)

    shared(t)
    pair_copy(n_kind).wait_recv()
    shared(2 * a + 1 - b)
    pair_sum(1, a).start()

    def act(s, g, u):
        hid[s] = (g / (1.0 + jnp.exp(-g)) * u).astype(bf16)

    pair_copy(0).wait_recv()
    pair_copy(1).wait_recv()
    close = (t, 2 * a + 1 - b)
    for c in range(CHUNKS):
        at = pl.ds(c * cols, cols)

        def wait_dispatch(d, _):
            dispatch_copy(c, d).wait_recv()
            return 0

        lax.fori_loop(1, ep, wait_dispatch, 0)
        for i, s in enumerate(close):
            g, u = dot(ld[:, at], gf[s, at, :]), dot(ld[:, at], uf[s, at, :])
            if c:
                g, u = g + acc[i, 0], u + acc[i, 1]
            if c < CHUNKS - 1:
                acc[i, 0] = g
                acc[i, 1] = u
            else:
                act(s, g, u)
        if c == 1:
            forward(0)
    wait_forwarded(0)
    rest = [near(d) for d in range(1, half)] + [near(d) + 1 - 2 * b for d in range(1, half)]
    gates = [dot(ld[...], gf[s]) for s in rest]
    forward(1)
    for n, s in enumerate(rest):
        if n == half - 1:
            wait_forwarded(1)
        act(s, gates[n], dot(ld[...], uf[s]))

    def back_copy(c, d):
        to = lax.rem(e + d, ep)
        at = pl.ds(c * cols, cols)
        return remote(
            rt.at[block(to), at], rv.at[block(e), at], b_send.at[c, d], b_recv.at[c, d], (to, t)
        )

    def near_copy(c, i):
        to = 4 * here + lax.rem(place4 + i, 4)
        at = pl.ds(c * cols, cols)
        return remote(
            rt.at[block(to), at], rv.at[block(e), at], hb_send.at[c, i], hb_recv.at[c, i], (to, t)
        )

    def gate_of(j):
        return 2 * (1 + here) + j % 2

    def gate_copy(c, j):
        at = pl.ds(c * cols, cols)
        return remote(
            rt.at[block(4 - 4 * here + j), at], g_blocks.at[j // 2, block(place4), at],
            g_send.at[c, j], g_recv.at[c, j // 2, place4], (gate_of(j), t),
        )

    def gate_arrival(c, i, r):
        at = pl.ds(c * cols, cols)
        return remote(
            rt.at[block(0), at], g_blocks.at[i, block(r), at],
            g_send.at[c, i], g_recv.at[c, i, r], (gate_of(0), t),
        )

    def row_copy(c, i):
        at = pl.ds(c * cols, cols)
        return remote(
            g_rows.at[i, :, at], g_in.at[:, at], m_send.at[c, i], m_recv.at[c],
            (4 - 4 * here + 2 * i + line, t),
        )

    def start_back(c):
        at = pl.ds(c * cols, cols)
        if chain and c < MERGED:
            for j in range(4):

                @pl.when(gate_of(j) != e)
                def _():
                    gate_copy(c, j).start()

                @pl.when(gate_of(j) == e)
                def _():
                    g_blocks[j // 2, block(place4), at] = rt[block(4 - 4 * here + j), at]

            for i in range(1, 4):
                near_copy(c, i).start()
        else:

            def start_one(d, _):
                back_copy(c, d).start()
                return 0

            lax.fori_loop(1, ep, start_one, 0)
        rv[block(e), at] = rt[block(e), at]

    def wait_back(c):
        if chain and c < MERGED:
            for i in range(1, 4):
                near_copy(c, i).wait_recv()
            row_copy(c, 0).wait_recv()
        else:

            def wait_one(d, _):
                back_copy(c, d).wait_recv()
                return 0

            lax.fori_loop(1, ep, wait_one, 0)

    def merge(c):
        if not chain or c >= MERGED:
            return
        at = pl.ds(c * cols, cols)

        @pl.when(is_gate)
        def _():
            for i in range(2):
                for r in range(1, 4):
                    gate_arrival(c, i, lax.rem(place4 + r, 4)).wait_recv()
                blocks = g_blocks[i, :, at]
                rows_in = dot(gate_mix[i, 0], blocks) + dot(gate_mix[i, 1], blocks)
                g_rows[i, :, at] = rows_in.astype(bf16)
                row_copy(c, i).start()

    if chain:
        mix = weighted(chosen, expert, own_routes, own_w)
        wide = 4 * cap
        for h in range(2):
            for n in range(2):
                own_mix[h, n] = mix[n][:, h * wide : (h + 1) * wide]

        @pl.when(is_gate)
        def _():
            for i in range(2):
                for c in table_copies(i):
                    c.wait_recv()
                named = g_routes[i]
                picked, which = table(named, 4 * here, 4)
                pair_of = weighted(picked, which, named, g_weights[i])
                for n in range(2):
                    gate_mix[i, n] = pair_of[n]

    for c in range(CHUNKS):
        k = 2 + c
        at = pl.ds(c * cols, cols)
        pair_copy(k).wait_recv()
        forward(k)
        wait_forwarded(k)
        total = dot(hid[0], df[0, :, at])
        for s in range(1, tp):
            total = total + dot(hid[s], df[s, :, at])
        rt[:, at] = total.astype(bf16)
        start_back(c)
        if c > 0:
            merge(c - 1)
        if c == NORMED_AT:
            start_far(0)
            forward(n_kind)
            for d in range(1, half):
                shared(near(d))
            wait_forwarded(n_kind)
            for d in range(1, half):
                shared(near(d) + 1 - 2 * b)
                pair_sum(1, lax.rem(a + half - d, half)).start()
            start_far(1)
    merge(CHUNKS - 1)

    if not chain:
        mix = weighted(chosen, expert, own_routes, own_w)
    pair_sum(1, a).wait_recv()
    for c in range(CHUNKS):
        at = pl.ds(c * cols, cols)
        wait_back(c)
        if chain:
            routed = jnp.zeros((rows, cols), f32)
            for h in (here, 1 - here)[: 1 if c < MERGED else 2]:
                got = rv[pl.ds(pl.multiple_of(h * wide, wide), wide), at]
                routed = routed + (dot(own_mix[h, 0], got) + dot(own_mix[h, 1], got))
            if c < MERGED:
                routed = routed + g_in[:, at].astype(f32)
        else:
            routed = dot(mix[0], rv[:, at]) + dot(mix[1], rv[:, at])
        exp_o[:, at] = (summed(1, c) + routed).astype(bf16)

    pair_sum(0, a).wait_recv()
    for c in range(CHUNKS):
        at = pl.ds(c * cols, cols)
        mix_o[:, at] = summed(0, c).astype(bf16)

    if chain:
        for c in table_copies(inner_level):
            c.wait_send()
        for c in range(MERGED):
            for j in range(4):

                @pl.when(gate_of(j) != e)
                def _():
                    gate_copy(c, j).wait_send()

            for i in range(1, 4):
                near_copy(c, i).wait_send()

            @pl.when(is_gate)
            def _():
                for i in range(2):
                    row_copy(c, i).wait_send()

    def sent(d, _):
        for c in range(CHUNKS):
            dispatch_copy(c, d).wait_send()
            if not chain or c >= MERGED:
                back_copy(c, d).wait_send()
        return 0

    lax.fori_loop(1, ep, sent, 0)
    for c in halos:
        c.wait_send()
    for k in range(kinds):
        pair_copy(k).wait_send()
        for d in range(1, half):
            x_copy(k, d).wait_send()
            forward_copy(k, d).wait_send()
    for j in range(2):
        for i in range(half):
            pair_sum(j, i).wait_send()
        for c in range(CHUNKS):
            for d in range(1, half):
                far_sum(j, d, c).wait_send()


def per_device(
    outer_gate, inner_gate, conv_values, conv_taps, out_weight, moe_input, norm_gain,
    gate_proj, up_proj, down_proj, shared_gate, shared_up, shared_down, routes, route_weight,
):
    tp = lax.axis_size("tp")
    ep = lax.axis_size("ep")
    half = tp // 2
    group, ch = inner_gate.shape
    rows, width = moe_input.shape
    units = gate_proj.shape[2]
    sh_units = shared_gate.shape[1]
    cap = 2 * rows * routes.shape[1] // ep
    cap = -(-cap // 16) * 16
    slots = ep * cap
    kinds = CHUNKS + 3
    vmem = pl.BlockSpec(memory_space=pltpu.VMEM)
    any_spec = pl.BlockSpec(memory_space=pl.ANY)
    dma = pltpu.SemaphoreType.DMA

    def buf(*shape):
        return pltpu.VMEM(shape, bf16)

    scratch = [
        buf(rows, width), buf(width), buf(*conv_taps.shape),
        pltpu.VMEM((routes.shape[1], group), jnp.int32), pltpu.VMEM((routes.shape[1], group), f32),
        buf(group, ch), buf(group, ch), buf(group, ch), buf(2, 16, ch),
        pltpu.VMEM((group + 16, ch), f32), buf(ch, width),
        buf(width, sh_units), buf(width, sh_units), buf(sh_units, width),
        buf(tp, width, units), buf(tp, width, units), buf(tp, units, width),
        buf(tp, rows, width), buf(slots, width), buf(slots, width),
        buf(tp, slots, units), buf(slots, width), buf(slots, width),
        pltpu.VMEM((2, 2, slots, units), f32), buf(2, tp, rows, width), buf(2, half, rows, width),
        buf(2, half - 1, rows, width), buf(2, half - 1, rows, width),
        dma((15,)), dma((2,)), dma((2,)), dma((kinds, half)), dma((kinds, half)),
        dma((kinds, tp)), dma((CHUNKS, ep)), dma((CHUNKS, ep)), dma((CHUNKS, ep)), dma((CHUNKS, ep)),
        dma((2, half)), dma((2, half)), dma((2, half, CHUNKS)), dma((2, half, CHUNKS)),
        pltpu.SemaphoreType.REGULAR((max(ep // 2 - 1, 1),)),
        pltpu.SemaphoreType.REGULAR((max(ep // 2 - 1, 1),)),
        pltpu.VMEM((2, routes.shape[1], rows), jnp.int32),
        pltpu.VMEM((2, routes.shape[1], rows), f32),
        buf(2, 4 * cap, width), buf(2, rows, width), buf(rows, width),
        buf(2, 2, rows, 4 * cap), buf(2, 2, rows, 4 * cap),
        dma((2,)), dma((2, 2)), dma((CHUNKS, 4)), dma((CHUNKS, 4)),
        dma((CHUNKS, 4)), dma((CHUNKS, 2, 4)), dma((CHUNKS, 2)), dma((CHUNKS,)),
    ]
    out = pltpu.VMEM((rows, width), bf16)
    return pl.pallas_call(
        functools.partial(kernel, (ep, tp, cap)),
        out_shape=(out, out),
        in_specs=[any_spec] * 15,
        out_specs=(vmem, vmem),
        scratch_shapes=scratch,
        compiler_params=pltpu.CompilerParams(
            collective_id=0, has_side_effects=True, vmem_limit_bytes=65536000
        ),
    )(
        outer_gate, inner_gate, conv_values, conv_taps, out_weight, moe_input,
        norm_gain, gate_proj, up_proj, down_proj,
        shared_gate, shared_up, shared_down, routes.T, route_weight.T,
    )


def solution(mesh):
    return jax.shard_map(
        per_device,
        mesh=mesh,
        in_specs=(
            P("ep", "tp"), P("ep", "tp"), P("ep", "tp"), P(None, "tp"), P("tp", None),
            P(("ep", "tp"), None), P(),
            P("ep", None, "tp"), P("ep", None, "tp"), P("ep", "tp", None),
            P(None, "tp"), P(None, "tp"), P("tp", None), P("ep", None), P("ep", None),
        ),
        out_specs=(P(("ep", "tp"), None), P(("ep", "tp"), None)),
        check_vma=False,
    )
```

```python
import functools

import jax
import jax.numpy as jnp
from jax import lax
from jax.experimental import pallas as pl
from jax.experimental.pallas import tpu as pltpu
from jax.sharding import PartitionSpec as P

epsilon = 1e-06
MESH = pl.DeviceIdType.MESH
f32 = jnp.float32
bf16 = jnp.bfloat16
CHUNKS = 4
NORMED_AT = 2
SPREAD_AT = 0
FAR_AT = 3


def dot(a, b):
    return jnp.dot(a, b, preferred_element_type=f32)


def kernel(
    dims,
    outer, inner, values, taps, out_w, tokens, gain, gate_p, up_p, down_p,
    sh_gate, sh_up, sh_down, routes, weights,
    mix_o, exp_o,
    l_tokens, l_gain, l_taps, l_routes, l_weights,
    l_outer, l_inner, l_values, halo, prod, l_out_w, l_sg, l_su, l_sd,
    gf, uf, df, nf, og, ld, hid, rt, rv,
    acc, parts, pairs, sums, arrived,
    loc_sem, sent_sem, halo_recv, t_recv,
    d_send, d_recv, b_send, b_recv, r_recv, rx_recv,
    ready_up, ready_down,
    g_routes, g_weights, g_blocks, g_rows, g_in, own_mix, gate_mix,
    gr_recv, b_in, g_recv,
    g_tokens, g_slots, gate_pick,
    d_in, raw_recv,
    far_g, far_u, far_d, sh_hid,
    px_recv, pn_recv, pg_recv, py_recv, pf_recv, pa_recv, pb_recv,
):
    ep, tp, cap = dims
    half = tp // 2
    e, t = lax.axis_index("ep"), lax.axis_index("tp")
    a, b = t // 2, lax.rem(t, 2)
    pair = (e, 2 * a + 1 - b)
    group, ch = l_inner.shape
    rows, width = tokens.shape
    slots = ep * cap
    cols = width // CHUNKS
    n_taps = taps.shape[0]

    def far(d):
        return 2 * lax.rem(a + d, half) + b

    def near(d):
        return 2 * lax.rem(a + half - d, half) + b

    def remote(src, dst, s, r, dev):
        return pltpu.make_async_remote_copy(
            src_ref=src, dst_ref=dst, send_sem=s, recv_sem=r, device_id=dev, device_id_type=MESH
        )

    barrier = pltpu.get_barrier_semaphore()

    def signal(sem, dev):
        pl.semaphore_signal(sem, inc=1, device_id=dev, device_id_type=MESH)

    levels = ep // 2
    level = e // 2
    below, above = level > 0, level < levels - 1
    lower, upper_dev = (jnp.maximum(e - 2, 0), t), (jnp.minimum(e + 2, ep - 1), t)
    signal(barrier, pair)
    for d in range(1, half):
        signal(barrier, (e, far(d)))
    chain = levels <= 4
    if chain:
        signal(barrier, (e + 1 - 2 * lax.rem(e, 2), t))

        @pl.when(below)
        def _():
            signal(barrier, lower)

        @pl.when(above)
        def _():
            signal(barrier, upper_dev)
    else:

        def greet(d, _):
            signal(barrier, (lax.rem(e + d, ep), t))
            return 0

        lax.fori_loop(1, ep, greet, 0)

    def ready_step(k):
        if not chain:
            return

        @pl.when(above)
        def _():
            signal(ready_up.at[k], upper_dev)

        @pl.when(below)
        def _():
            signal(ready_down.at[k], lower)

        @pl.when(below)
        def _():
            pl.semaphore_wait(ready_up.at[k], 1)

        @pl.when(above)
        def _():
            pl.semaphore_wait(ready_down.at[k], 1)

    small = [
        pltpu.make_async_copy(s, d, loc_sem.at[10 + i])
        for i, (s, d) in enumerate(
            (
                (tokens, l_tokens), (gain, l_gain), (routes, l_routes), (weights, l_weights),
                (taps, l_taps),
            )
        )
    ]
    for c in small:
        c.start()
    local = [
        pltpu.make_async_copy(s, d, loc_sem.at[i])
        for i, (s, d) in enumerate(
            (
                (inner, l_inner), (values, l_values), (outer, l_outer), (out_w, l_out_w),
                (sh_gate, l_sg), (sh_up, l_su), (sh_down, l_sd),
                (gate_p.at[0], gf.at[t]), (up_p.at[0], uf.at[t]), (down_p.at[0], df.at[t]),
            )
        )
    ]
    for c in local:
        c.start()

    if chain:
        pl.semaphore_wait(barrier, half + 1 + below.astype(jnp.int32) + above.astype(jnp.int32))
    else:
        pl.semaphore_wait(barrier, half + ep - 1)

    kinds = CHUNKS + 3
    n_kind = kinds - 1

    def land(k, s):
        if k == 0:
            return gf.at[s]
        if k == 1:
            return uf.at[s]
        if k == n_kind:
            return nf.at[s]
        return df.at[s, :, pl.ds((k - 2) * cols, cols)]

    def origin(k):
        if k == 0:
            return gate_p.at[0]
        if k == 1:
            return up_p.at[0]
        if k == n_kind:
            return nf.at[t]
        return down_p.at[0, :, pl.ds((k - 2) * cols, cols)]

    to_gate, to_slots, to_back, to_rows, to_pieces, to_spread, to_forward = range(7)
    to_x, to_pair, to_relay, to_sums, to_halo, to_table = 7, 8, 9, 10, 11, 13

    def group_of(i):
        return sent_sem.at[i]

    def drain(i, ref):
        remote(ref, ref, group_of(i), group_of(i), pair).wait_send()

    def x_copy(k, d):
        return remote(origin(k), land(k, t), group_of(to_x), t_recv.at[k, d], (e, far(d)))

    def pair_copy(k):
        return remote(origin(k), land(k, t), group_of(to_gate if chain and k == n_kind else to_pair), t_recv.at[k, 0], pair)

    def forward_copy(k, d):
        s = near(d)
        return remote(land(k, s), land(k, s), group_of(to_relay), t_recv.at[k, half - 1 + d], pair)

    def start_x(k):
        for d in range(1, half):
            x_copy(k, d).start()

    def forward(k):
        for d in range(1, half):
            x_copy(k, d).wait_recv()
            forward_copy(k, d).start()

    def wait_forwarded(k):
        for d in range(1, half):
            forward_copy(k, d).wait_recv()

    here = e // 4
    place4 = lax.rem(e, 4)
    line = lax.rem(e, 2)
    inner_level = lax.rem(level, 2)
    is_gate = level == 1 + here
    other_gate = (jnp.minimum(2 * (2 - here) + line, ep - 1), t)
    beside = (e + 1 - 2 * line, t)
    partner_e = e + 2 - 4 * inner_level
    partner = (jnp.minimum(partner_e, ep - 1), t)

    def away(i, y):
        return 4 - 4 * here + 2 * i + y

    unit = sh_down.shape[0] // ep

    def piece(w, d, i):
        ref = (far_g, far_u, far_d)[w].at[d - 1]
        n = ref.shape[0] // ep
        return ref.at[pl.ds(pl.multiple_of(i * n, n), n), :]

    def piece_x(w, d):
        src = (sh_gate, sh_up, sh_down)[w]
        n = src.shape[0] // ep
        return remote(
            src.at[pl.ds(pl.multiple_of(e * n, n), n), :], piece(w, d, e),
            group_of(to_pieces), px_recv.at[w, d - 1], (e, far(d)),
        )

    def piece_partner(w, d, i):
        return remote(piece(w, d, i), piece(w, d, i), group_of(to_spread), pn_recv.at[w, d - 1], partner)

    beside_e = e + 1 - 2 * line

    def piece_gate(w, d, k):
        p = piece(w, d, (e, beside_e)[k])
        arrived_sem = pa_recv.at[d - 1] if k else pg_recv.at[w, d - 1]
        return remote(p, p, group_of(to_spread), arrived_sem, other_gate)

    def piece_forward(w, d, i):
        p = piece(w, d, away(i, line))
        return remote(p, p, group_of(to_forward), pf_recv.at[w, d - 1], partner)

    def piece_beside(w, d, j):
        p = piece(w, d, (e, partner_e, away(0, line), away(1, line))[j])
        arrived_sem = py_recv.at[d - 1] if j else pb_recv.at[w, d - 1]
        return remote(p, p, group_of(to_pieces), arrived_sem, beside)

    pieces = [(w, d) for w in range(3) for d in range(1, half)] if chain else []

    def spread_own():
        for w, d in pieces:
            piece_x(w, d).wait_recv()
            piece_gate(w, d, 0).start()
            piece_partner(w, d, e).start()
            piece_beside(w, d, 0).start()

    def spread_partner():
        for w, d in pieces:
            piece_beside(w, d, 0).wait_recv()
            piece_gate(w, d, 1).start()
        for w, d in pieces:
            piece_partner(w, d, partner_e).wait_recv()
            piece_beside(w, d, 1).start()

    def spread_away(gates):
        @pl.when(is_gate if gates else jnp.logical_not(is_gate))
        def _():
            for w, d in pieces:
                n = (far_g, far_u, far_d)[w].shape[1] // ep
                both = (far_g, far_u, far_d)[w].at[d - 1, pl.ds(0, 2 * n), :]
                arrived_sem = (pg_recv if gates else pf_recv).at[w, d - 1]
                remote(both, both, group_of(to_spread), arrived_sem, partner).wait_recv()
                for i in range(2):
                    if gates:
                        piece_forward(w, d, i).start()
                    else:
                        piece_beside(w, d, 2 + i).start()

    def wait_pieces():
        for d in range(1, half):

            @pl.when(is_gate)
            def _():
                for count, sem in ((3, py_recv), (6, pa_recv)):
                    some = og.at[pl.ds(0, count * unit), :]
                    remote(some, some, group_of(to_pieces), sem.at[d - 1], beside).wait_recv()

            @pl.when(jnp.logical_not(is_gate))
            def _():
                some = og.at[pl.ds(0, 9 * unit), :]
                remote(some, some, group_of(to_pieces), py_recv.at[d - 1], beside).wait_recv()

    if chain:
        for w, d in pieces:
            piece_x(w, d).start()
    for k in range(n_kind if chain else 3 + NORMED_AT):
        start_x(k)
    ready_step(0)
    for c in small:
        c.wait()
    mine = pl.ds(pl.multiple_of(t * rows, rows), rows)
    own_routes, own_w = l_routes[:, mine], l_weights[:, mine]

    def table(named, first, count):
        slot = lax.broadcasted_iota(jnp.int32, (count * cap, rows), 0)
        index = slot // cap
        place = (slot - index * cap).astype(f32)
        expert = index + first
        hit = jnp.zeros((count * cap, rows), f32)
        for k in range(named.shape[0]):
            hit = jnp.where(named[k : k + 1, :] == expert, 1.0, hit)
        upper = lax.broadcasted_iota(jnp.int32, (rows, rows), 0) < lax.broadcasted_iota(
            jnp.int32, (rows, rows), 1
        )
        earlier = dot(hit.astype(bf16), jnp.where(upper, 1.0, 0.0).astype(bf16))
        return jnp.where(earlier == place, hit, 0.0), expert

    def weighted(chosen, expert, named, given):
        scale = jnp.zeros(chosen.shape, f32)
        for k in range(named.shape[0]):
            scale = jnp.where(named[k : k + 1, :] == expert, given[k : k + 1, :], scale)
        full = jnp.transpose(chosen * scale)
        high = full.astype(bf16)
        return high, (full - high.astype(f32)).astype(bf16)

    chosen, expert = table(own_routes, 0, ep)
    sender = chosen.astype(bf16)

    if levels > 2:
        ready_step(1)
    scales = l_gain[...].astype(f32).reshape(1, width)

    def norm_rows(i, _):
        at = pl.ds(pl.multiple_of(i * 16, 16), 16)
        v = l_tokens[at, :].astype(f32)
        square = jnp.mean(v * v, axis=-1, keepdims=True)
        nf[t, at, :] = (v * lax.rsqrt(square + epsilon) * scales).astype(bf16)
        return 0

    lax.fori_loop(0, rows // 16, norm_rows, 0)

    for k in range(2, levels - 1):
        ready_step(k)

    def table_copies(i):
        return [
            remote(src.at[:, mine], dst.at[i], group_of(to_table + n), gr_recv.at[n], other_gate)
            for n, (src, dst) in enumerate(((l_routes, g_routes), (l_weights, g_weights)))
        ]

    edge = pl.ds(group - 16, 16)
    halos = [
        remote(src.at[edge, :], halo.at[i], group_of(to_halo + i), halo_recv.at[i], (lax.rem(e + 1, ep), t))
        for i, src in enumerate((inner, values))
    ]
    for c in halos:
        c.start()
    if chain:
        for c in table_copies(inner_level):
            c.start()

    def block(i):
        return pl.ds(pl.multiple_of(i * cap, cap), cap)

    def near_dispatch(c, i):
        to = 4 * here + lax.rem(place4 + i, 4)
        at = pl.ds(c * cols, cols)
        return remote(
            og.at[block(to), at], ld.at[block(e), at], group_of(to_gate), d_in.at[c], (to, t)
        )

    def raw_copy(c, i):
        at = pl.ds(c * cols, cols)
        return remote(
            nf.at[t, :, at], g_tokens.at[i, :, at], group_of(to_gate), raw_recv.at[c], other_gate
        )

    def slot_copy(c, i, r):
        at = pl.ds(c * cols, cols)
        return remote(
            g_slots.at[i, block(r), at], ld.at[block(away(i, line)), at],
            group_of(to_slots), d_in.at[c], (4 * here + r, t),
        )

    def forward_slots(c):
        if not chain:
            return
        at = pl.ds(c * cols, cols)

        @pl.when(is_gate)
        def _():
            both = g_slots.at[0, pl.ds(0, 2 * rows), at]
            remote(both, both, group_of(to_gate), raw_recv.at[c], other_gate).wait_recv()
            for i in range(2):
                g_slots[i, :, at] = dot(gate_pick[i], g_tokens[i, :, at]).astype(bf16)
                for r in range(4):

                    @pl.when(place4 != r)
                    def _():
                        slot_copy(c, i, r).start()

                ld[block(away(i, line)), at] = g_slots[i, block(place4), at]

    def dispatch_copy(c, d):
        to = lax.rem(e + d, ep)
        at = pl.ds(c * cols, cols)
        return remote(
            og.at[block(to), at], ld.at[block(e), at], d_send.at[c, d], d_recv.at[c, d], (to, t)
        )

    for c in range(CHUNKS):
        at = pl.ds(c * cols, cols)
        og[:, at] = dot(sender, nf[t, :, at]).astype(bf16)

        if chain:
            raw_copy(c, inner_level).start()
            for i in range(1, 4):
                near_dispatch(c, i).start()
        else:

            def start_dispatch(d, _):
                dispatch_copy(c, d).start()
                return 0

            lax.fori_loop(1, ep, start_dispatch, 0)
        ld[block(e), at] = og[block(e), at]
    if not chain:
        start_x(n_kind)
    for k in range(kinds):
        pair_copy(k).start()
    if chain:
        spread_own()
    else:
        for k in range(3 + NORMED_AT, n_kind):
            start_x(k)


    def pair_sum(j, i):
        return remote(
            parts.at[j, 2 * i + 1 - b], pairs.at[j, i], group_of(to_sums), r_recv.at[j, i], pair
        )

    def far_sum(j, d, c):
        at = pl.ds(c * cols, cols)
        return remote(
            sums.at[j, d - 1, :, at], arrived.at[j, d - 1, :, at],
            group_of(to_sums), rx_recv.at[j, d - 1, c], (e, far(d)),
        )

    def start_far(j):
        for d in range(1, half):
            i = lax.rem(a + d, half)
            pair_sum(j, i).wait_recv()
            for c in range(CHUNKS):
                at = pl.ds(c * cols, cols)
                total = parts[j, 2 * i + b, :, at].astype(f32) + pairs[j, i, :, at].astype(f32)
                sums[j, d - 1, :, at] = total.astype(bf16)
                far_sum(j, d, c).start()

    def summed(j, c):
        at = pl.ds(c * cols, cols)
        total = parts[j, t, :, at].astype(f32) + pairs[j, a, :, at].astype(f32)
        if chain and j == 1:
            return total
        for d in range(1, half):
            far_sum(j, d, c).wait_recv()
        for d in range(1, half):
            total = total + arrived[j, d - 1, :, at].astype(f32)
        return total

    if chain:
        mix = weighted(chosen, expert, own_routes, own_w)
        wide = 4 * cap
        for h in range(2):
            for n in range(2):
                own_mix[h, n] = mix[n][:, h * wide : (h + 1) * wide]

        @pl.when(is_gate)
        def _():
            for n, ref in enumerate((g_routes, g_weights)):
                remote(ref, ref, group_of(to_table + n), gr_recv.at[n], other_gate).wait_recv()
            for i in range(2):
                named = g_routes[i]
                picked, which = table(named, 4 * here, 4)
                pair_of = weighted(picked, which, named, g_weights[i])
                gate_pick[i] = picked.astype(bf16)
                for n in range(2):
                    gate_mix[i, n] = pair_of[n]

    for c in local[:4]:
        c.wait()
    for c in halos:
        c.wait_recv()
    before = halo[0].astype(f32) * halo[1].astype(f32)
    prod[0:16, :] = jnp.where(e > 0, before, 0.0)
    prod[16:, :] = l_inner[...].astype(f32) * l_values[...].astype(f32)
    tap = l_taps[...].astype(f32)
    for s in range(tp):
        lo = s * rows
        conv = jnp.zeros((rows, ch), f32)
        for j in range(n_taps):
            first = 16 + lo - (n_taps - 1) + j
            conv = conv + tap[j : j + 1, :] * prod[first : first + rows, :]
        gated = (l_outer[lo : lo + rows, :].astype(f32) * conv).astype(bf16)
        for c in range(CHUNKS):
            at = pl.ds(c * cols, cols)
            parts[0, s, :, at] = dot(gated, l_out_w[:, at]).astype(bf16)
        if s == tp // 2 - 1:
            forward_slots(0)
    for i in range(half):
        pair_sum(0, i).start()
    forward_slots(1)

    for c in local[4:]:
        c.wait()

    def shared(s):
        x = nf[s]
        g = dot(x, l_sg[...])
        u = dot(x, l_su[...])
        h = (g / (1.0 + jnp.exp(-g)) * u).astype(bf16)
        for c in range(CHUNKS):
            at = pl.ds(c * cols, cols)
            parts[1, s, :, at] = dot(h, l_sd[:, at]).astype(bf16)

    def shared_hidden(x, gate_w, up_w):
        g = dot(x, gate_w)
        u = dot(x, up_w)
        return (g / (1.0 + jnp.exp(-g)) * u).astype(bf16)

    couple = (t, 2 * a + 1 - b)
    if chain:
        sh_hid[0, 0] = shared_hidden(nf[t], l_sg[...], l_su[...])
        forward_slots(2)
        pair_copy(n_kind).wait_recv()
        sh_hid[0, 1] = shared_hidden(nf[couple[1]], l_sg[...], l_su[...])
        forward_slots(3)
        spread_partner()
        spread_away(True)
    else:
        shared(t)
        pair_copy(n_kind).wait_recv()
        shared(couple[1])
        pair_sum(1, a).start()

    def far_shared():
        wait_pieces()
        for i, s in enumerate(couple):
            for d in range(1, half):
                sh_hid[d, i] = shared_hidden(nf[s], far_g[d - 1], far_u[d - 1])
        for i in (1, 0):
            for c in range(CHUNKS):
                at = pl.ds(c * cols, cols)
                total = dot(sh_hid[0, i], l_sd[:, at])
                for d in range(1, half):
                    total = total + dot(sh_hid[d, i], far_d[d - 1, :, at])
                parts[1, couple[i], :, at] = total.astype(bf16)
            if i:
                pair_sum(1, a).start()

    def act(s, g, u):
        hid[s] = (g / (1.0 + jnp.exp(-g)) * u).astype(bf16)

    pair_copy(0).wait_recv()
    pair_copy(1).wait_recv()
    close = (t, 2 * a + 1 - b)
    for c in range(CHUNKS):
        at = pl.ds(c * cols, cols)

        if chain:
            for count, mine_too in ((5, is_gate), (7, jnp.logical_not(is_gate))):

                @pl.when(mine_too)
                def _():
                    blocks = ld.at[pl.ds(0, count * cap), at]
                    remote(blocks, blocks, group_of(to_gate), d_in.at[c], pair).wait_recv()

        else:

            def wait_dispatch(d, _):
                dispatch_copy(c, d).wait_recv()
                return 0

            lax.fori_loop(1, ep, wait_dispatch, 0)
        for i, s in enumerate(close):
            g, u = dot(ld[:, at], gf[s, at, :]), dot(ld[:, at], uf[s, at, :])
            if c:
                g, u = g + acc[i, 0], u + acc[i, 1]
            if c < CHUNKS - 1:
                acc[i, 0] = g
                acc[i, 1] = u
            else:
                act(s, g, u)
        if c == 1:
            forward(0)
    wait_forwarded(0)
    rest = [near(d) for d in range(1, half)] + [near(d) + 1 - 2 * b for d in range(1, half)]
    gates = [dot(ld[...], gf[s]) for s in rest]
    forward(1)
    for n, s in enumerate(rest):
        if n == half - 1:
            wait_forwarded(1)
        act(s, gates[n], dot(ld[...], uf[s]))

    def back_copy(c, d):
        to = lax.rem(e + d, ep)
        at = pl.ds(c * cols, cols)
        return remote(
            rt.at[block(to), at], rv.at[block(e), at], b_send.at[c, d], b_recv.at[c, d], (to, t)
        )

    def near_copy(c, i):
        to = e + (0, 1 - 2 * line, 2 - 4 * inner_level, 3 - 2 * line - 4 * inner_level)[i]
        at = pl.ds(c * cols, cols)
        return remote(
            rt.at[block(to), at], rv.at[block(e), at], group_of(to_back), b_in.at[c], (to, t)
        )

    def gate_of(j):
        return 2 * (1 + here) + j % 2

    def gate_copy(c, j):
        at = pl.ds(c * cols, cols)
        return remote(
            rt.at[block(4 - 4 * here + j), at], g_blocks.at[j // 2, block(place4), at],
            group_of(to_back), g_recv.at[c], (gate_of(j), t),
        )

    def row_copy(c, i):
        at = pl.ds(c * cols, cols)
        return remote(
            g_rows.at[i, :, at], g_in.at[:, at], group_of(to_rows), b_in.at[c],
            (4 - 4 * here + 2 * i + line, t),
        )

    def start_back(c):
        at = pl.ds(c * cols, cols)
        if chain:
            for j in range(4):

                @pl.when(gate_of(j) != e)
                def _():
                    gate_copy(c, j).start()

                @pl.when(gate_of(j) == e)
                def _():
                    g_blocks[j // 2, block(place4), at] = rt[block(4 - 4 * here + j), at]

            for gate, now in ((True, (2, 3)), (False, (1,))):

                @pl.when(is_gate if gate else jnp.logical_not(is_gate))
                def _():
                    for i in now:
                        near_copy(c, i).start()
                    for m in range(CHUNKS if c == CHUNKS - 1 else 0):
                        for i in range(1, 4):
                            if i not in now:
                                near_copy(m, i).start()

        else:

            def start_one(d, _):
                back_copy(c, d).start()
                return 0

            lax.fori_loop(1, ep, start_one, 0)
        rv[block(e), at] = rt[block(e), at]

    def wait_back(c):
        if chain:
            got = rt.at[pl.ds(0, 3 * cap + rows), pl.ds(c * cols, cols)]
            remote(got, got, group_of(to_back), b_in.at[c], pair).wait_recv()
        else:

            def wait_one(d, _):
                back_copy(c, d).wait_recv()
                return 0

            lax.fori_loop(1, ep, wait_one, 0)

    def merge(c):
        if not chain:
            return
        at = pl.ds(c * cols, cols)

        @pl.when(is_gate)
        def _():
            six = rt.at[pl.ds(0, 6 * cap), at]
            remote(six, six, group_of(to_back), g_recv.at[c], pair).wait_recv()
            for i in range(2):
                blocks = g_blocks[i, :, at]
                rows_in = dot(gate_mix[i, 0], blocks) + dot(gate_mix[i, 1], blocks)
                g_rows[i, :, at] = rows_in.astype(bf16)
                row_copy(c, i).start()

    for c in range(CHUNKS):
        k = 2 + c
        at = pl.ds(c * cols, cols)
        pair_copy(k).wait_recv()
        forward(k)
        wait_forwarded(k)
        total = dot(hid[0], df[0, :, at])
        for s in range(1, tp):
            total = total + dot(hid[s], df[s, :, at])
        rt[:, at] = total.astype(bf16)
        start_back(c)
        if c > 0:
            merge(c - 1)
        if chain and c == 1:
            start_far(0)
        if chain and c == FAR_AT:
            far_shared()
        if chain and c == SPREAD_AT:
            spread_away(False)
        if not chain and c == NORMED_AT:
            start_far(0)
            forward(n_kind)
            for d in range(1, half):
                shared(near(d))
            wait_forwarded(n_kind)
            for d in range(1, half):
                shared(near(d) + 1 - 2 * b)
                pair_sum(1, lax.rem(a + half - d, half)).start()
            start_far(1)
    merge(CHUNKS - 1)

    if not chain:
        mix = weighted(chosen, expert, own_routes, own_w)
    pair_sum(1, a).wait_recv()
    for c in range(CHUNKS):
        if c == CHUNKS - 1:
            pair_sum(0, a).wait_recv()
            for m in range(CHUNKS):
                at = pl.ds(m * cols, cols)
                mix_o[:, at] = summed(0, m).astype(bf16)
        at = pl.ds(c * cols, cols)
        wait_back(c)
        if chain:
            got = rv[pl.ds(pl.multiple_of(here * wide, wide), wide), at]
            routed = dot(own_mix[here, 0], got) + dot(own_mix[here, 1], got)
            routed = routed + g_in[:, at].astype(f32)
        else:
            routed = dot(mix[0], rv[:, at]) + dot(mix[1], rv[:, at])
        exp_o[:, at] = (summed(1, c) + routed).astype(bf16)


    for c in halos:
        c.wait_send()
    if chain:
        for c in table_copies(inner_level):
            c.wait_send()
        drain(to_gate, og.at[pl.ds(0, 2 * rows + 3 * cap), :])
        drain(to_spread, og.at[pl.ds(0, 9 * unit), :])
        drain(to_x, gf.at[pl.ds(0, 3)])
        drain(to_pair, gf.at[pl.ds(0, 3)])
        drain(to_relay, gf.at[pl.ds(0, 3)])
        drain(to_sums, og.at[pl.ds(0, 4 * rows), :])

        @pl.when(is_gate)
        def _():
            drain(to_slots, og.at[pl.ds(0, 6 * cap), :])
            drain(to_rows, og.at[pl.ds(0, 2 * rows), :])
            drain(to_forward, og.at[pl.ds(0, 6 * unit), :])
            drain(to_back, og.at[pl.ds(0, 5 * cap), :])
            drain(to_pieces, og.at[pl.ds(0, 9 * unit), :])

        @pl.when(jnp.logical_not(is_gate))
        def _():
            drain(to_back, og.at[pl.ds(0, 7 * cap), :])
            drain(to_pieces, og.at[pl.ds(0, 15 * unit), :])

        return

    def sent(d, _):
        for c in range(CHUNKS):
            dispatch_copy(c, d).wait_send()
            back_copy(c, d).wait_send()
        return 0

    lax.fori_loop(1, ep, sent, 0)
    for k in range(kinds):
        pair_copy(k).wait_send()
        for d in range(1, half):
            x_copy(k, d).wait_send()
            forward_copy(k, d).wait_send()
    for j in range(2):
        for i in range(half):
            pair_sum(j, i).wait_send()
        for c in range(CHUNKS):
            for d in range(1, half):
                far_sum(j, d, c).wait_send()


def per_device(
    outer_gate, inner_gate, conv_values, conv_taps, out_weight, moe_input, norm_gain,
    gate_proj, up_proj, down_proj, shared_gate, shared_up, shared_down, routes, route_weight,
):
    tp = lax.axis_size("tp")
    ep = lax.axis_size("ep")
    half = tp // 2
    group, ch = inner_gate.shape
    rows, width = moe_input.shape
    units = gate_proj.shape[2]
    sh_units = shared_gate.shape[1]
    cap = 2 * rows * routes.shape[1] // ep
    cap = -(-cap // 16) * 16
    slots = ep * cap
    kinds = CHUNKS + 3
    vmem = pl.BlockSpec(memory_space=pltpu.VMEM)
    any_spec = pl.BlockSpec(memory_space=pl.ANY)
    dma = pltpu.SemaphoreType.DMA

    direct = (1, 1) if ep <= 8 else (CHUNKS, ep)

    def buf(*shape):
        return pltpu.VMEM(shape, bf16)

    scratch = [
        buf(rows, width), buf(width), buf(*conv_taps.shape),
        pltpu.VMEM((routes.shape[1], group), jnp.int32), pltpu.VMEM((routes.shape[1], group), f32),
        buf(group, ch), buf(group, ch), buf(group, ch), buf(2, 16, ch),
        pltpu.VMEM((group + 16, ch), f32), buf(ch, width),
        buf(width, sh_units), buf(width, sh_units), buf(sh_units, width),
        buf(tp, width, units), buf(tp, width, units), buf(tp, units, width),
        buf(tp, rows, width), buf(slots, width), buf(slots, width),
        buf(tp, slots, units), buf(slots, width), buf(slots, width),
        pltpu.VMEM((2, 2, slots, units), f32), buf(2, tp, rows, width), buf(2, half, rows, width),
        buf(2, half - 1, rows, width), buf(2, half - 1, rows, width),
        dma((15,)), dma((15,)), dma((2,)),
        dma((kinds, 2 * half - 1)), dma(direct), dma(direct), dma(direct), dma(direct),
        dma((2, half)), dma((2, half - 1, CHUNKS)),
        pltpu.SemaphoreType.REGULAR((max(ep // 2 - 1, 1),)),
        pltpu.SemaphoreType.REGULAR((max(ep // 2 - 1, 1),)),
        pltpu.VMEM((2, routes.shape[1], rows), jnp.int32),
        pltpu.VMEM((2, routes.shape[1], rows), f32),
        buf(2, 4 * cap, width), buf(2, rows, width), buf(rows, width),
        buf(2, 2, rows, 4 * cap), buf(2, 2, rows, 4 * cap),
        dma((2,)), dma((CHUNKS,)), dma((CHUNKS,)),
        buf(2, rows, width), buf(2, 4 * cap, width), buf(2, 4 * cap, rows),
        dma((CHUNKS,)), dma((CHUNKS,)),
        buf(half - 1, width, sh_units), buf(half - 1, width, sh_units), buf(half - 1, sh_units, width),
        buf(half, 2, rows, sh_units),
        dma((3, half - 1)), dma((3, half - 1)), dma((3, half - 1)), dma((half - 1,)), dma((3, half - 1)),
        dma((half - 1,)), dma((3, half - 1)),
    ]
    out = pltpu.VMEM((rows, width), bf16)
    return pl.pallas_call(
        functools.partial(kernel, (ep, tp, cap)),
        out_shape=(out, out),
        in_specs=[any_spec] * 15,
        out_specs=(vmem, vmem),
        scratch_shapes=scratch,
        compiler_params=pltpu.CompilerParams(
            collective_id=0, has_side_effects=True, vmem_limit_bytes=65536000
        ),
    )(
        outer_gate, inner_gate, conv_values, conv_taps, out_weight, moe_input,
        norm_gain, gate_proj, up_proj, down_proj,
        shared_gate, shared_up, shared_down, routes.T, route_weight.T,
    )


def solution(mesh):
    return jax.shard_map(
        per_device,
        mesh=mesh,
        in_specs=(
            P("ep", "tp"), P("ep", "tp"), P("ep", "tp"), P(None, "tp"), P("tp", None),
            P(("ep", "tp"), None), P(),
            P("ep", None, "tp"), P("ep", None, "tp"), P("ep", "tp", None),
            P(None, "tp"), P(None, "tp"), P("tp", None), P("ep", None), P("ep", None),
        ),
        out_specs=(P(("ep", "tp"), None), P(("ep", "tp"), None)),
        check_vma=False,
    )
```

```python
import functools

import jax
import jax.numpy as jnp
from jax import lax
from jax.experimental import pallas as pl
from jax.experimental.pallas import tpu as pltpu
from jax.sharding import PartitionSpec as P

epsilon = 1e-06
MESH = pl.DeviceIdType.MESH
f32 = jnp.float32
bf16 = jnp.bfloat16
CHUNKS = 4
RETURNS = 8
LAG = 3
NORMED_AT = 2
SPREAD_AT = 2


def dot(a, b):
    return jnp.dot(a, b, preferred_element_type=f32)


def kernel(
    dims,
    outer, inner, values, taps, out_w, tokens, gain, gate_p, up_p, down_p,
    sh_gate, sh_up, sh_down, routes, weights,
    mix_o, exp_o,
    l_tokens, l_gain, l_taps, l_routes, l_weights,
    l_outer, l_inner, l_values, halo, prod, l_out_w, l_sg, l_su, l_sd,
    gf, uf, df, nf, og, ld, hid, rt, rv,
    acc, parts, pairs, sums, arrived,
    loc_sem, sent_sem, halo_recv, t_recv,
    d_send, d_recv, b_send, b_recv, r_recv, rx_recv,
    ready_up, ready_down,
    g_routes, g_weights, g_blocks, g_rows, g_in, own_mix, gate_mix,
    gr_recv, b_in, g_recv,
    g_tokens, g_slots, gate_pick,
    d_in, raw_recv,
    far_g, far_u, far_d, sh_hid,
    px_recv, pn_recv, pg_recv, py_recv, pf_recv, pa_recv, pb_recv,
):
    ep, tp, cap = dims
    half = tp // 2
    e, t = lax.axis_index("ep"), lax.axis_index("tp")
    a, b = t // 2, lax.rem(t, 2)
    pair = (e, 2 * a + 1 - b)
    group, ch = l_inner.shape
    rows, width = tokens.shape
    slots = ep * cap
    cols = width // CHUNKS
    returns = RETURNS if ep <= 8 else CHUNKS
    lag = LAG if ep <= 8 else 1
    bcols = width // returns
    n_taps = taps.shape[0]

    def far(d):
        return 2 * lax.rem(a + d, half) + b

    def near(d):
        return 2 * lax.rem(a + half - d, half) + b

    def remote(src, dst, s, r, dev):
        return pltpu.make_async_remote_copy(
            src_ref=src, dst_ref=dst, send_sem=s, recv_sem=r, device_id=dev, device_id_type=MESH
        )

    barrier = pltpu.get_barrier_semaphore()

    def signal(sem, dev):
        pl.semaphore_signal(sem, inc=1, device_id=dev, device_id_type=MESH)

    levels = ep // 2
    level = e // 2
    below, above = level > 0, level < levels - 1
    lower, upper_dev = (jnp.maximum(e - 2, 0), t), (jnp.minimum(e + 2, ep - 1), t)
    signal(barrier, pair)
    for d in range(1, half):
        signal(barrier, (e, far(d)))
    chain = levels <= 4
    if chain:
        signal(barrier, (e + 1 - 2 * lax.rem(e, 2), t))

        @pl.when(below)
        def _():
            signal(barrier, lower)

        @pl.when(above)
        def _():
            signal(barrier, upper_dev)
    else:

        def greet(d, _):
            signal(barrier, (lax.rem(e + d, ep), t))
            return 0

        lax.fori_loop(1, ep, greet, 0)

    def ready_step(k):
        if not chain:
            return

        @pl.when(above)
        def _():
            signal(ready_up.at[k], upper_dev)

        @pl.when(below)
        def _():
            signal(ready_down.at[k], lower)

        @pl.when(below)
        def _():
            pl.semaphore_wait(ready_up.at[k], 1)

        @pl.when(above)
        def _():
            pl.semaphore_wait(ready_down.at[k], 1)

    small = [
        pltpu.make_async_copy(s, d, loc_sem.at[10 + i])
        for i, (s, d) in enumerate(
            (
                (tokens, l_tokens), (gain, l_gain), (routes, l_routes), (weights, l_weights),
                (taps, l_taps),
            )
        )
    ]
    for c in small:
        c.start()
    local = [
        pltpu.make_async_copy(s, d, loc_sem.at[i])
        for i, (s, d) in enumerate(
            (
                (inner, l_inner), (values, l_values), (outer, l_outer), (out_w, l_out_w),
                (sh_gate, l_sg), (sh_up, l_su), (sh_down, l_sd),
                (gate_p.at[0], gf.at[t]), (up_p.at[0], uf.at[t]), (down_p.at[0], df.at[t]),
            )
        )
    ]
    for c in local:
        c.start()

    if chain:
        pl.semaphore_wait(barrier, half + 1 + below.astype(jnp.int32) + above.astype(jnp.int32))
    else:
        pl.semaphore_wait(barrier, half + ep - 1)

    kinds = returns + 3
    n_kind = kinds - 1

    def land(k, s):
        if k == 0:
            return gf.at[s]
        if k == 1:
            return uf.at[s]
        if k == n_kind:
            return nf.at[s]
        return df.at[s, :, pl.ds((k - 2) * bcols, bcols)]

    def origin(k):
        if k == 0:
            return gate_p.at[0]
        if k == 1:
            return up_p.at[0]
        if k == n_kind:
            return nf.at[t]
        return down_p.at[0, :, pl.ds((k - 2) * bcols, bcols)]

    to_gate, to_slots, to_back, to_rows, to_pieces, to_spread, to_forward = range(7)
    to_x, to_pair, to_relay, to_sums, to_halo, to_table = 7, 8, 9, 10, 11, 13

    def group_of(i):
        return sent_sem.at[i]

    def drain(i, ref):
        remote(ref, ref, group_of(i), group_of(i), pair).wait_send()

    def x_copy(k, d):
        return remote(origin(k), land(k, t), group_of(to_x), t_recv.at[k, d], (e, far(d)))

    def pair_copy(k):
        return remote(origin(k), land(k, t), group_of(to_gate if chain and k == n_kind else to_pair), t_recv.at[k, 0], pair)

    def forward_copy(k, d):
        s = near(d)
        return remote(land(k, s), land(k, s), group_of(to_relay), t_recv.at[k, half - 1 + d], pair)

    def start_x(k):
        for d in range(1, half):
            x_copy(k, d).start()

    def forward(k):
        for d in range(1, half):
            x_copy(k, d).wait_recv()
            forward_copy(k, d).start()

    def wait_forwarded(k):
        for d in range(1, half):
            forward_copy(k, d).wait_recv()

    here = e // 4
    place4 = lax.rem(e, 4)
    line = lax.rem(e, 2)
    inner_level = lax.rem(level, 2)
    is_gate = level == 1 + here
    other_gate = (jnp.minimum(2 * (2 - here) + line, ep - 1), t)
    beside = (e + 1 - 2 * line, t)
    partner_e = e + 2 - 4 * inner_level
    partner = (jnp.minimum(partner_e, ep - 1), t)

    def away(i, y):
        return 4 - 4 * here + 2 * i + y

    unit = sh_down.shape[0] // ep

    def piece(w, d, i):
        ref = (far_g, far_u, far_d)[w].at[d - 1]
        n = ref.shape[0] // ep
        return ref.at[pl.ds(pl.multiple_of(i * n, n), n), :]

    def piece_x(w, d):
        src = (sh_gate, sh_up, sh_down)[w]
        n = src.shape[0] // ep
        return remote(
            src.at[pl.ds(pl.multiple_of(e * n, n), n), :], piece(w, d, e),
            group_of(to_pieces), px_recv.at[w, d - 1], (e, far(d)),
        )

    def piece_partner(w, d, i):
        return remote(piece(w, d, i), piece(w, d, i), group_of(to_spread), pn_recv.at[w, d - 1], partner)

    beside_e = e + 1 - 2 * line

    def piece_gate(w, d, k):
        p = piece(w, d, (e, beside_e)[k])
        arrived_sem = pa_recv.at[d - 1] if k else pg_recv.at[w, d - 1]
        return remote(p, p, group_of(to_spread), arrived_sem, other_gate)

    def piece_forward(w, d, i):
        p = piece(w, d, away(i, line))
        return remote(p, p, group_of(to_forward), pf_recv.at[w, d - 1], partner)

    def piece_beside(w, d, j):
        p = piece(w, d, (e, partner_e, away(0, line), away(1, line))[j])
        arrived_sem = py_recv.at[d - 1] if j else pb_recv.at[w, d - 1]
        return remote(p, p, group_of(to_pieces), arrived_sem, beside)

    pieces = [(w, d) for w in range(3) for d in range(1, half)] if chain else []

    def spread_own():
        for w, d in pieces:
            piece_x(w, d).wait_recv()
            piece_gate(w, d, 0).start()
            piece_partner(w, d, e).start()
            piece_beside(w, d, 0).start()

    def spread_partner():
        for w, d in pieces:
            piece_beside(w, d, 0).wait_recv()
            piece_gate(w, d, 1).start()
        for w, d in pieces:
            piece_partner(w, d, partner_e).wait_recv()
            piece_beside(w, d, 1).start()

    def spread_away(gates):
        @pl.when(is_gate if gates else jnp.logical_not(is_gate))
        def _():
            for w, d in pieces:
                n = (far_g, far_u, far_d)[w].shape[1] // ep
                both = (far_g, far_u, far_d)[w].at[d - 1, pl.ds(0, 2 * n), :]
                arrived_sem = (pg_recv if gates else pf_recv).at[w, d - 1]
                remote(both, both, group_of(to_spread), arrived_sem, partner).wait_recv()
                for i in range(2):
                    if gates:
                        piece_forward(w, d, i).start()
                    else:
                        piece_beside(w, d, 2 + i).start()

    def wait_pieces():
        for d in range(1, half):

            @pl.when(is_gate)
            def _():
                for count, sem in ((3, py_recv), (6, pa_recv)):
                    some = og.at[pl.ds(0, count * unit), :]
                    remote(some, some, group_of(to_pieces), sem.at[d - 1], beside).wait_recv()

            @pl.when(jnp.logical_not(is_gate))
            def _():
                some = og.at[pl.ds(0, 9 * unit), :]
                remote(some, some, group_of(to_pieces), py_recv.at[d - 1], beside).wait_recv()

    if chain:
        for w, d in pieces:
            piece_x(w, d).start()
    for k in range(n_kind if chain else 3 + NORMED_AT):
        start_x(k)
    ready_step(0)
    for c in small:
        c.wait()
    mine = pl.ds(pl.multiple_of(t * rows, rows), rows)
    own_routes, own_w = l_routes[:, mine], l_weights[:, mine]

    def table(named, first, count):
        slot = lax.broadcasted_iota(jnp.int32, (count * cap, rows), 0)
        index = slot // cap
        place = (slot - index * cap).astype(f32)
        expert = index + first
        hit = jnp.zeros((count * cap, rows), f32)
        for k in range(named.shape[0]):
            hit = jnp.where(named[k : k + 1, :] == expert, 1.0, hit)
        upper = lax.broadcasted_iota(jnp.int32, (rows, rows), 0) < lax.broadcasted_iota(
            jnp.int32, (rows, rows), 1
        )
        earlier = dot(hit.astype(bf16), jnp.where(upper, 1.0, 0.0).astype(bf16))
        return jnp.where(earlier == place, hit, 0.0), expert

    def weighted(chosen, expert, named, given):
        scale = jnp.zeros(chosen.shape, f32)
        for k in range(named.shape[0]):
            scale = jnp.where(named[k : k + 1, :] == expert, given[k : k + 1, :], scale)
        full = jnp.transpose(chosen * scale)
        high = full.astype(bf16)
        return high, (full - high.astype(f32)).astype(bf16)

    chosen, expert = table(own_routes, 0, ep)
    sender = chosen.astype(bf16)

    if levels > 2:
        ready_step(1)
    scales = l_gain[...].astype(f32).reshape(1, width)

    def norm_rows(i, _):
        at = pl.ds(pl.multiple_of(i * 16, 16), 16)
        v = l_tokens[at, :].astype(f32)
        square = jnp.mean(v * v, axis=-1, keepdims=True)
        nf[t, at, :] = (v * lax.rsqrt(square + epsilon) * scales).astype(bf16)
        return 0

    lax.fori_loop(0, rows // 16, norm_rows, 0)

    for k in range(2, levels - 1):
        ready_step(k)

    def table_copies(i):
        return [
            remote(src.at[:, mine], dst.at[i], group_of(to_table + n), gr_recv.at[n], other_gate)
            for n, (src, dst) in enumerate(((l_routes, g_routes), (l_weights, g_weights)))
        ]

    edge = pl.ds(group - 16, 16)
    halos = [
        remote(src.at[edge, :], halo.at[i], group_of(to_halo + i), halo_recv.at[i], (lax.rem(e + 1, ep), t))
        for i, src in enumerate((inner, values))
    ]
    for c in halos:
        c.start()
    if chain:
        for c in table_copies(inner_level):
            c.start()

    def block(i):
        return pl.ds(pl.multiple_of(i * cap, cap), cap)

    def near_dispatch(c, i):
        to = 4 * here + lax.rem(place4 + i, 4)
        at = pl.ds(c * cols, cols)
        return remote(
            og.at[block(to), at], ld.at[block(e), at], group_of(to_gate), d_in.at[c], (to, t)
        )

    def raw_copy(c, i):
        at = pl.ds(c * cols, cols)
        return remote(
            nf.at[t, :, at], g_tokens.at[i, :, at], group_of(to_gate), raw_recv.at[c], other_gate
        )

    def slot_copy(c, i, r):
        at = pl.ds(c * cols, cols)
        return remote(
            g_slots.at[i, block(r), at], ld.at[block(away(i, line)), at],
            group_of(to_slots), d_in.at[c], (4 * here + r, t),
        )

    def forward_slots(c):
        if not chain:
            return
        at = pl.ds(c * cols, cols)

        @pl.when(is_gate)
        def _():
            both = g_slots.at[0, pl.ds(0, 2 * rows), at]
            remote(both, both, group_of(to_gate), raw_recv.at[c], other_gate).wait_recv()
            for i in range(2):
                g_slots[i, :, at] = dot(gate_pick[i], g_tokens[i, :, at]).astype(bf16)
                for r in range(4):

                    @pl.when(place4 != r)
                    def _():
                        slot_copy(c, i, r).start()

                ld[block(away(i, line)), at] = g_slots[i, block(place4), at]

    def dispatch_copy(c, d):
        to = lax.rem(e + d, ep)
        at = pl.ds(c * cols, cols)
        return remote(
            og.at[block(to), at], ld.at[block(e), at], d_send.at[c, d], d_recv.at[c, d], (to, t)
        )

    for c in range(CHUNKS):
        at = pl.ds(c * cols, cols)
        og[:, at] = dot(sender, nf[t, :, at]).astype(bf16)

        if chain:
            raw_copy(c, inner_level).start()
            for i in range(1, 4):
                near_dispatch(c, i).start()
        else:

            def start_dispatch(d, _):
                dispatch_copy(c, d).start()
                return 0

            lax.fori_loop(1, ep, start_dispatch, 0)
        ld[block(e), at] = og[block(e), at]
    if not chain:
        start_x(n_kind)
    for k in range(kinds):
        pair_copy(k).start()
    if chain:
        spread_own()
    else:
        for k in range(3 + NORMED_AT, n_kind):
            start_x(k)


    def pair_sum(j, i):
        return remote(
            parts.at[j, 2 * i + 1 - b], pairs.at[j, i], group_of(to_sums), r_recv.at[j, i], pair
        )

    def far_sum(j, d, c):
        at = pl.ds(c * cols, cols)
        return remote(
            sums.at[j, d - 1, :, at], arrived.at[j, d - 1, :, at],
            group_of(to_sums), rx_recv.at[j, d - 1, c], (e, far(d)),
        )

    def start_far(j):
        for d in range(1, half):
            i = lax.rem(a + d, half)
            pair_sum(j, i).wait_recv()
            for c in range(CHUNKS):
                at = pl.ds(c * cols, cols)
                total = parts[j, 2 * i + b, :, at].astype(f32) + pairs[j, i, :, at].astype(f32)
                sums[j, d - 1, :, at] = total.astype(bf16)
                far_sum(j, d, c).start()

    def own_shared(at):
        return parts[1, t, :, at].astype(f32) + pairs[1, a, :, at].astype(f32)

    def summed(j, c):
        at = pl.ds(c * cols, cols)
        total = parts[j, t, :, at].astype(f32) + pairs[j, a, :, at].astype(f32)
        for d in range(1, half):
            far_sum(j, d, c).wait_recv()
        for d in range(1, half):
            total = total + arrived[j, d - 1, :, at].astype(f32)
        return total

    if chain:
        mix = weighted(chosen, expert, own_routes, own_w)
        wide = 4 * cap
        for h in range(2):
            for n in range(2):
                own_mix[h, n] = mix[n][:, h * wide : (h + 1) * wide]

        @pl.when(is_gate)
        def _():
            for n, ref in enumerate((g_routes, g_weights)):
                remote(ref, ref, group_of(to_table + n), gr_recv.at[n], other_gate).wait_recv()
            for i in range(2):
                named = g_routes[i]
                picked, which = table(named, 4 * here, 4)
                pair_of = weighted(picked, which, named, g_weights[i])
                gate_pick[i] = picked.astype(bf16)
                for n in range(2):
                    gate_mix[i, n] = pair_of[n]

    for c in local[:4]:
        c.wait()
    for c in halos:
        c.wait_recv()
    before = halo[0].astype(f32) * halo[1].astype(f32)
    prod[0:16, :] = jnp.where(e > 0, before, 0.0)
    prod[16:, :] = l_inner[...].astype(f32) * l_values[...].astype(f32)
    tap = l_taps[...].astype(f32)
    for s in range(tp):
        lo = s * rows
        conv = jnp.zeros((rows, ch), f32)
        for j in range(n_taps):
            first = 16 + lo - (n_taps - 1) + j
            conv = conv + tap[j : j + 1, :] * prod[first : first + rows, :]
        gated = (l_outer[lo : lo + rows, :].astype(f32) * conv).astype(bf16)
        for c in range(CHUNKS):
            at = pl.ds(c * cols, cols)
            parts[0, s, :, at] = dot(gated, l_out_w[:, at]).astype(bf16)
        if s == tp // 2 - 1:
            forward_slots(0)
    for i in range(half):
        pair_sum(0, i).start()
    forward_slots(1)

    for c in local[4:]:
        c.wait()

    def shared(s):
        x = nf[s]
        g = dot(x, l_sg[...])
        u = dot(x, l_su[...])
        h = (g / (1.0 + jnp.exp(-g)) * u).astype(bf16)
        for c in range(CHUNKS):
            at = pl.ds(c * cols, cols)
            parts[1, s, :, at] = dot(h, l_sd[:, at]).astype(bf16)

    def shared_hidden(x, gate_w, up_w):
        g = dot(x, gate_w)
        u = dot(x, up_w)
        return (g / (1.0 + jnp.exp(-g)) * u).astype(bf16)

    couple = (t, 2 * a + 1 - b)
    if chain:
        sh_hid[0, 0] = shared_hidden(nf[t], l_sg[...], l_su[...])
        forward_slots(2)
        pair_copy(n_kind).wait_recv()
        sh_hid[0, 1] = shared_hidden(nf[couple[1]], l_sg[...], l_su[...])
        forward_slots(3)
        spread_partner()
        spread_away(True)
    else:
        shared(t)
        pair_copy(n_kind).wait_recv()
        shared(couple[1])
        pair_sum(1, a).start()

    def far_shared():
        wait_pieces()
        for i in (1, 0):
            for d in range(1, half):
                sh_hid[d, i] = shared_hidden(nf[couple[i]], far_g[d - 1], far_u[d - 1])
            for c in range(CHUNKS):
                at = pl.ds(c * cols, cols)
                total = dot(sh_hid[0, i], l_sd[:, at])
                for d in range(1, half):
                    total = total + dot(sh_hid[d, i], far_d[d - 1, :, at])
                parts[1, couple[i], :, at] = total.astype(bf16)
            if i:
                pair_sum(1, a).start()

    def act(s, g, u):
        hid[s] = (g / (1.0 + jnp.exp(-g)) * u).astype(bf16)

    pair_copy(0).wait_recv()
    pair_copy(1).wait_recv()
    close = (t, 2 * a + 1 - b)
    for c in range(CHUNKS):
        at = pl.ds(c * cols, cols)

        if chain:
            for count, mine_too in ((5, is_gate), (7, jnp.logical_not(is_gate))):

                @pl.when(mine_too)
                def _():
                    blocks = ld.at[pl.ds(0, count * cap), at]
                    remote(blocks, blocks, group_of(to_gate), d_in.at[c], pair).wait_recv()

        else:

            def wait_dispatch(d, _):
                dispatch_copy(c, d).wait_recv()
                return 0

            lax.fori_loop(1, ep, wait_dispatch, 0)
        for i, s in enumerate(close):
            g, u = dot(ld[:, at], gf[s, at, :]), dot(ld[:, at], uf[s, at, :])
            if c:
                g, u = g + acc[i, 0], u + acc[i, 1]
            if c < CHUNKS - 1:
                acc[i, 0] = g
                acc[i, 1] = u
            else:
                act(s, g, u)
        if c == 1:
            forward(0)
    wait_forwarded(0)
    rest = [near(d) for d in range(1, half)] + [near(d) + 1 - 2 * b for d in range(1, half)]
    gates = [dot(ld[...], gf[s]) for s in rest]
    forward(1)
    for n, s in enumerate(rest):
        if n == half - 1:
            wait_forwarded(1)
        act(s, gates[n], dot(ld[...], uf[s]))

    def back_copy(c, d):
        to = lax.rem(e + d, ep)
        at = pl.ds(c * bcols, bcols)
        return remote(
            rt.at[block(to), at], rv.at[block(e), at], b_send.at[c, d], b_recv.at[c, d], (to, t)
        )

    def near_copy(c, i):
        to = e + (0, 1 - 2 * line, 2 - 4 * inner_level, 3 - 2 * line - 4 * inner_level)[i]
        at = pl.ds(c * bcols, bcols)
        return remote(
            rt.at[block(to), at], rv.at[block(e), at], group_of(to_back), b_in.at[c], (to, t)
        )

    def gate_of(j):
        return 2 * (1 + here) + j % 2

    def gate_copy(c, j):
        at = pl.ds(c * bcols, bcols)
        return remote(
            rt.at[block(4 - 4 * here + j), at], g_blocks.at[j // 2, block(place4), at],
            group_of(to_back), g_recv.at[c], (gate_of(j), t),
        )

    def row_copy(c, i):
        at = pl.ds(c * bcols, bcols)
        return remote(
            g_rows.at[i, :, at], g_in.at[:, at], group_of(to_rows), b_in.at[c],
            (4 - 4 * here + 2 * i + line, t),
        )

    def start_back(c):
        at = pl.ds(c * bcols, bcols)
        if chain:
            for j in range(4):

                @pl.when(gate_of(j) != e)
                def _():
                    gate_copy(c, j).start()

                @pl.when(gate_of(j) == e)
                def _():
                    g_blocks[j // 2, block(place4), at] = rt[block(4 - 4 * here + j), at]

            for gate, now in ((True, (2, 3)), (False, (1,))):

                @pl.when(is_gate if gate else jnp.logical_not(is_gate))
                def _():
                    for i in now:
                        near_copy(c, i).start()
                    for m in range(returns if c == returns - 1 else 0):
                        for i in range(1, 4):
                            if i not in now:
                                near_copy(m, i).start()

        else:

            def start_one(d, _):
                back_copy(c, d).start()
                return 0

            lax.fori_loop(1, ep, start_one, 0)
        rv[block(e), at] = rt[block(e), at]

    def wait_back(c):
        if chain:
            got = rt.at[pl.ds(0, 3 * cap + rows), pl.ds(c * bcols, bcols)]
            remote(got, got, group_of(to_back), b_in.at[c], pair).wait_recv()
        else:

            def wait_one(d, _):
                back_copy(c, d).wait_recv()
                return 0

            lax.fori_loop(1, ep, wait_one, 0)

    def merge(c):
        if not chain:
            return
        at = pl.ds(c * bcols, bcols)

        @pl.when(is_gate)
        def _():
            six = rt.at[pl.ds(0, 6 * cap), at]
            remote(six, six, group_of(to_back), g_recv.at[c], pair).wait_recv()
            for i in range(2):
                blocks = g_blocks[i, :, at]
                rows_in = dot(gate_mix[i, 0], blocks) + dot(gate_mix[i, 1], blocks)
                g_rows[i, :, at] = rows_in.astype(bf16)
                row_copy(c, i).start()

    for c in range(returns):
        k = 2 + c
        at = pl.ds(c * bcols, bcols)
        pair_copy(k).wait_recv()
        forward(k)
        wait_forwarded(k)
        total = dot(hid[0], df[0, :, at])
        for s in range(1, tp):
            total = total + dot(hid[s], df[s, :, at])
        rt[:, at] = total.astype(bf16)
        start_back(c)
        if c >= lag:
            merge(c - lag)
        if chain and c == 1:
            start_far(0)
        if chain and c == SPREAD_AT:
            spread_away(False)
        if not chain and c == NORMED_AT:
            start_far(0)
            forward(n_kind)
            for d in range(1, half):
                shared(near(d))
            wait_forwarded(n_kind)
            for d in range(1, half):
                shared(near(d) + 1 - 2 * b)
                pair_sum(1, lax.rem(a + half - d, half)).start()
            start_far(1)
    for c in range(returns - lag, returns):
        merge(c)
    if chain:
        far_shared()

    if not chain:
        mix = weighted(chosen, expert, own_routes, own_w)
    pair_sum(1, a).wait_recv()
    for c in range(returns):
        if c == returns - 1:
            pair_sum(0, a).wait_recv()
            for m in range(CHUNKS):
                at = pl.ds(m * cols, cols)
                mix_o[:, at] = summed(0, m).astype(bf16)
        at = pl.ds(c * bcols, bcols)
        wait_back(c)
        if chain:
            got = rv[pl.ds(pl.multiple_of(here * wide, wide), wide), at]
            routed = dot(own_mix[here, 0], got) + dot(own_mix[here, 1], got)
            routed = routed + g_in[:, at].astype(f32)
        else:
            routed = dot(mix[0], rv[:, at]) + dot(mix[1], rv[:, at])
        exp_o[:, at] = ((own_shared(at) if chain else summed(1, c)) + routed).astype(bf16)


    for c in halos:
        c.wait_send()
    if chain:
        for c in table_copies(inner_level):
            c.wait_send()
        drain(to_gate, og.at[pl.ds(0, 2 * rows + 3 * cap), :])
        drain(to_spread, og.at[pl.ds(0, 9 * unit), :])
        drain(to_x, gf.at[pl.ds(0, 3)])
        drain(to_pair, gf.at[pl.ds(0, 3)])
        drain(to_relay, gf.at[pl.ds(0, 3)])
        drain(to_sums, og.at[pl.ds(0, 4 * rows), :])

        @pl.when(is_gate)
        def _():
            drain(to_slots, og.at[pl.ds(0, 6 * cap), :])
            drain(to_rows, og.at[pl.ds(0, 2 * rows), :])
            drain(to_forward, og.at[pl.ds(0, 6 * unit), :])
            drain(to_back, og.at[pl.ds(0, 5 * cap), :])
            drain(to_pieces, og.at[pl.ds(0, 9 * unit), :])

        @pl.when(jnp.logical_not(is_gate))
        def _():
            drain(to_back, og.at[pl.ds(0, 7 * cap), :])
            drain(to_pieces, og.at[pl.ds(0, 15 * unit), :])

        return

    def sent(d, _):
        for c in range(CHUNKS):
            dispatch_copy(c, d).wait_send()
            back_copy(c, d).wait_send()
        return 0

    lax.fori_loop(1, ep, sent, 0)
    for k in range(kinds):
        pair_copy(k).wait_send()
        for d in range(1, half):
            x_copy(k, d).wait_send()
            forward_copy(k, d).wait_send()
    for j in range(2):
        for i in range(half):
            pair_sum(j, i).wait_send()
        for c in range(CHUNKS):
            for d in range(1, half):
                far_sum(j, d, c).wait_send()


def per_device(
    outer_gate, inner_gate, conv_values, conv_taps, out_weight, moe_input, norm_gain,
    gate_proj, up_proj, down_proj, shared_gate, shared_up, shared_down, routes, route_weight,
):
    tp = lax.axis_size("tp")
    ep = lax.axis_size("ep")
    half = tp // 2
    group, ch = inner_gate.shape
    rows, width = moe_input.shape
    units = gate_proj.shape[2]
    sh_units = shared_gate.shape[1]
    cap = 2 * rows * routes.shape[1] // ep
    cap = -(-cap // 16) * 16
    slots = ep * cap
    returns = RETURNS if ep <= 8 else CHUNKS
    kinds = returns + 3
    vmem = pl.BlockSpec(memory_space=pltpu.VMEM)
    any_spec = pl.BlockSpec(memory_space=pl.ANY)
    dma = pltpu.SemaphoreType.DMA

    direct = (1, 1) if ep <= 8 else (CHUNKS, ep)

    def buf(*shape):
        return pltpu.VMEM(shape, bf16)

    scratch = [
        buf(rows, width), buf(width), buf(*conv_taps.shape),
        pltpu.VMEM((routes.shape[1], group), jnp.int32), pltpu.VMEM((routes.shape[1], group), f32),
        buf(group, ch), buf(group, ch), buf(group, ch), buf(2, 16, ch),
        pltpu.VMEM((group + 16, ch), f32), buf(ch, width),
        buf(width, sh_units), buf(width, sh_units), buf(sh_units, width),
        buf(tp, width, units), buf(tp, width, units), buf(tp, units, width),
        buf(tp, rows, width), buf(slots, width), buf(slots, width),
        buf(tp, slots, units), buf(slots, width), buf(slots, width),
        pltpu.VMEM((2, 2, slots, units), f32), buf(2, tp, rows, width), buf(2, half, rows, width),
        buf(2, half - 1, rows, width), buf(2, half - 1, rows, width),
        dma((15,)), dma((15,)), dma((2,)),
        dma((kinds, 2 * half - 1)), dma(direct), dma(direct), dma(direct), dma(direct),
        dma((2, half)), dma((2, half - 1, CHUNKS)),
        pltpu.SemaphoreType.REGULAR((max(ep // 2 - 1, 1),)),
        pltpu.SemaphoreType.REGULAR((max(ep // 2 - 1, 1),)),
        pltpu.VMEM((2, routes.shape[1], rows), jnp.int32),
        pltpu.VMEM((2, routes.shape[1], rows), f32),
        buf(2, 4 * cap, width), buf(2, rows, width), buf(rows, width),
        buf(2, 2, rows, 4 * cap), buf(2, 2, rows, 4 * cap),
        dma((2,)), dma((returns,)), dma((returns,)),
        buf(2, rows, width), buf(2, 4 * cap, width), buf(2, 4 * cap, rows),
        dma((CHUNKS,)), dma((CHUNKS,)),
        buf(half - 1, width, sh_units), buf(half - 1, width, sh_units), buf(half - 1, sh_units, width),
        buf(half, 2, rows, sh_units),
        dma((3, half - 1)), dma((3, half - 1)), dma((3, half - 1)), dma((half - 1,)), dma((3, half - 1)),
        dma((half - 1,)), dma((3, half - 1)),
    ]
    out = pltpu.VMEM((rows, width), bf16)
    return pl.pallas_call(
        functools.partial(kernel, (ep, tp, cap)),
        out_shape=(out, out),
        in_specs=[any_spec] * 15,
        out_specs=(vmem, vmem),
        scratch_shapes=scratch,
        compiler_params=pltpu.CompilerParams(
            collective_id=0, has_side_effects=True, vmem_limit_bytes=65536000
        ),
    )(
        outer_gate, inner_gate, conv_values, conv_taps, out_weight, moe_input,
        norm_gain, gate_proj, up_proj, down_proj,
        shared_gate, shared_up, shared_down, routes.T, route_weight.T,
    )


def solution(mesh):
    return jax.shard_map(
        per_device,
        mesh=mesh,
        in_specs=(
            P("ep", "tp"), P("ep", "tp"), P("ep", "tp"), P(None, "tp"), P("tp", None),
            P(("ep", "tp"), None), P(),
            P("ep", None, "tp"), P("ep", None, "tp"), P("ep", "tp", None),
            P(None, "tp"), P(None, "tp"), P("tp", None), P("ep", None), P("ep", None),
        ),
        out_specs=(P(("ep", "tp"), None), P(("ep", "tp"), None)),
        check_vma=False,
    )
```

```python
import functools

import jax
import jax.numpy as jnp
from jax import lax
from jax.experimental import pallas as pl
from jax.experimental.pallas import tpu as pltpu
from jax.sharding import PartitionSpec as P

epsilon = 1e-06
MESH = pl.DeviceIdType.MESH
f32 = jnp.float32
bf16 = jnp.bfloat16
CHUNKS = 4
RETURNS = 8
LAG = 3
NORMED_AT = 2
SPREAD_AT = 2


def dot(a, b):
    return jnp.dot(a, b, preferred_element_type=f32)


def kernel(
    dims,
    outer, inner, values, taps, out_w, tokens, gain, gate_p, up_p, down_p,
    sh_gate, sh_up, sh_down, routes, weights,
    mix_o, exp_o,
    l_tokens, l_gain, l_taps, l_routes, l_weights,
    l_outer, l_inner, l_values, halo, prod, l_out_w, l_sg, l_su, l_sd,
    gf, uf, df, nf, og, ld, hid, rt, rv,
    acc, parts, pairs, sums, arrived,
    loc_sem, sent_sem, halo_recv, t_recv,
    d_send, d_recv, b_send, b_recv, r_recv, rx_recv,
    ready_up, ready_down,
    g_routes, g_weights, g_blocks, g_rows, g_in, own_mix, gate_mix,
    gr_recv, b_in, g_recv,
    g_tokens, g_slots, gate_pick,
    d_in, raw_recv,
    far_g, far_u, far_d, sh_hid,
    px_recv, pn_recv, pg_recv, py_recv, pf_recv, pa_recv, pb_recv,
):
    ep, tp, cap = dims
    half = tp // 2
    e, t = lax.axis_index("ep"), lax.axis_index("tp")
    a, b = t // 2, lax.rem(t, 2)
    pair = (e, 2 * a + 1 - b)
    group, ch = l_inner.shape
    rows, width = tokens.shape
    slots = ep * cap
    cols = width // CHUNKS
    returns = RETURNS if ep <= 8 else CHUNKS
    lag = LAG if ep <= 8 else 1
    bcols = width // returns
    n_taps = taps.shape[0]

    def far(d):
        return 2 * lax.rem(a + d, half) + b

    def near(d):
        return 2 * lax.rem(a + half - d, half) + b

    def remote(src, dst, s, r, dev):
        return pltpu.make_async_remote_copy(
            src_ref=src, dst_ref=dst, send_sem=s, recv_sem=r, device_id=dev, device_id_type=MESH
        )

    barrier = pltpu.get_barrier_semaphore()

    def signal(sem, dev):
        pl.semaphore_signal(sem, inc=1, device_id=dev, device_id_type=MESH)

    levels = ep // 2
    level = e // 2
    below, above = level > 0, level < levels - 1
    lower, upper_dev = (jnp.maximum(e - 2, 0), t), (jnp.minimum(e + 2, ep - 1), t)
    signal(barrier, pair)
    for d in range(1, half):
        signal(barrier, (e, far(d)))
    chain = levels <= 4
    if chain:
        signal(barrier, (e + 1 - 2 * lax.rem(e, 2), t))

        @pl.when(below)
        def _():
            signal(barrier, lower)

        @pl.when(above)
        def _():
            signal(barrier, upper_dev)
    else:

        def greet(d, _):
            signal(barrier, (lax.rem(e + d, ep), t))
            return 0

        lax.fori_loop(1, ep, greet, 0)

    def ready_step(k):
        if not chain:
            return

        @pl.when(above)
        def _():
            signal(ready_up.at[k], upper_dev)

        @pl.when(below)
        def _():
            signal(ready_down.at[k], lower)

        @pl.when(below)
        def _():
            pl.semaphore_wait(ready_up.at[k], 1)

        @pl.when(above)
        def _():
            pl.semaphore_wait(ready_down.at[k], 1)

    small = [
        pltpu.make_async_copy(s, d, loc_sem.at[10 + i])
        for i, (s, d) in enumerate(
            (
                (tokens, l_tokens), (gain, l_gain), (routes, l_routes), (weights, l_weights),
                (taps, l_taps),
            )
        )
    ]
    for c in small:
        c.start()
    local = [
        pltpu.make_async_copy(s, d, loc_sem.at[i])
        for i, (s, d) in enumerate(
            (
                (inner, l_inner), (values, l_values), (outer, l_outer), (out_w, l_out_w),
                (sh_gate, l_sg), (sh_up, l_su), (sh_down, l_sd),
                (gate_p.at[0], gf.at[t]), (up_p.at[0], uf.at[t]), (down_p.at[0], df.at[t]),
            )
        )
    ]
    for c in local:
        c.start()

    if chain:
        pl.semaphore_wait(barrier, half + 1 + below.astype(jnp.int32) + above.astype(jnp.int32))
    else:
        pl.semaphore_wait(barrier, half + ep - 1)

    kinds = returns + 3
    n_kind = kinds - 1

    def land(k, s):
        if k == 0:
            return gf.at[s]
        if k == 1:
            return uf.at[s]
        if k == n_kind:
            return nf.at[s]
        return df.at[s, :, pl.ds((k - 2) * bcols, bcols)]

    def origin(k):
        if k == 0:
            return gate_p.at[0]
        if k == 1:
            return up_p.at[0]
        if k == n_kind:
            return nf.at[t]
        return down_p.at[0, :, pl.ds((k - 2) * bcols, bcols)]

    to_gate, to_slots, to_back, to_rows, to_pieces, to_spread, to_forward = range(7)
    to_x, to_pair, to_relay, to_sums, to_halo, to_table = 7, 8, 9, 10, 11, 13

    def group_of(i):
        return sent_sem.at[i]

    def drain(i, ref):
        remote(ref, ref, group_of(i), group_of(i), pair).wait_send()

    def x_copy(k, d):
        return remote(origin(k), land(k, t), group_of(to_x), t_recv.at[k, d], (e, far(d)))

    def pair_copy(k):
        return remote(origin(k), land(k, t), group_of(to_gate if chain and k == n_kind else to_pair), t_recv.at[k, 0], pair)

    def forward_copy(k, d):
        s = near(d)
        return remote(land(k, s), land(k, s), group_of(to_relay), t_recv.at[k, half - 1 + d], pair)

    def start_x(k):
        for d in range(1, half):
            x_copy(k, d).start()

    def forward(k):
        for d in range(1, half):
            x_copy(k, d).wait_recv()
            forward_copy(k, d).start()

    def wait_forwarded(k):
        for d in range(1, half):
            forward_copy(k, d).wait_recv()

    here = e // 4
    place4 = lax.rem(e, 4)
    line = lax.rem(e, 2)
    inner_level = lax.rem(level, 2)
    is_gate = level == 1 + here
    other_gate = (jnp.minimum(2 * (2 - here) + line, ep - 1), t)
    beside = (e + 1 - 2 * line, t)
    partner_e = e + 2 - 4 * inner_level
    partner = (jnp.minimum(partner_e, ep - 1), t)

    def away(i, y):
        return 4 - 4 * here + 2 * i + y

    unit = sh_down.shape[0] // ep

    def piece(w, d, i):
        ref = (far_g, far_u, far_d)[w].at[d - 1]
        n = ref.shape[0] // ep
        return ref.at[pl.ds(pl.multiple_of(i * n, n), n), :]

    def piece_x(w, d):
        src = (sh_gate, sh_up, sh_down)[w]
        n = src.shape[0] // ep
        return remote(
            src.at[pl.ds(pl.multiple_of(e * n, n), n), :], piece(w, d, e),
            group_of(to_pieces), px_recv.at[w, d - 1], (e, far(d)),
        )

    def piece_partner(w, d, i):
        return remote(piece(w, d, i), piece(w, d, i), group_of(to_spread), pn_recv.at[w, d - 1], partner)

    beside_e = e + 1 - 2 * line

    def piece_gate(w, d, k):
        p = piece(w, d, (e, beside_e)[k])
        arrived_sem = pa_recv.at[d - 1] if k else pg_recv.at[w, d - 1]
        return remote(p, p, group_of(to_spread), arrived_sem, other_gate)

    def piece_forward(w, d, i):
        p = piece(w, d, away(i, line))
        return remote(p, p, group_of(to_forward), pf_recv.at[w, d - 1], partner)

    def piece_beside(w, d, j):
        p = piece(w, d, (e, partner_e, away(0, line), away(1, line))[j])
        arrived_sem = py_recv.at[d - 1] if j else pb_recv.at[w, d - 1]
        return remote(p, p, group_of(to_pieces), arrived_sem, beside)

    pieces = [(w, d) for w in range(3) for d in range(1, half)] if chain else []

    def spread_own():
        for w, d in pieces:
            piece_x(w, d).wait_recv()
            piece_gate(w, d, 0).start()
            piece_partner(w, d, e).start()
            piece_beside(w, d, 0).start()

    def spread_partner():
        for w, d in pieces:
            piece_beside(w, d, 0).wait_recv()
            piece_gate(w, d, 1).start()
        for w, d in pieces:
            piece_partner(w, d, partner_e).wait_recv()
            piece_beside(w, d, 1).start()

    def spread_away(gates):
        @pl.when(is_gate if gates else jnp.logical_not(is_gate))
        def _():
            for w, d in pieces:
                n = (far_g, far_u, far_d)[w].shape[1] // ep
                both = (far_g, far_u, far_d)[w].at[d - 1, pl.ds(0, 2 * n), :]
                arrived_sem = (pg_recv if gates else pf_recv).at[w, d - 1]
                remote(both, both, group_of(to_spread), arrived_sem, partner).wait_recv()
                for i in range(2):
                    if gates:
                        piece_forward(w, d, i).start()
                    else:
                        piece_beside(w, d, 2 + i).start()

    def wait_pieces():
        for d in range(1, half):

            @pl.when(is_gate)
            def _():
                for count, sem in ((3, py_recv), (6, pa_recv)):
                    some = og.at[pl.ds(0, count * unit), :]
                    remote(some, some, group_of(to_pieces), sem.at[d - 1], beside).wait_recv()

            @pl.when(jnp.logical_not(is_gate))
            def _():
                some = og.at[pl.ds(0, 9 * unit), :]
                remote(some, some, group_of(to_pieces), py_recv.at[d - 1], beside).wait_recv()

    if chain:
        for w, d in pieces:
            piece_x(w, d).start()
    for k in range(n_kind if chain else 3 + NORMED_AT):
        start_x(k)
    ready_step(0)
    for c in small:
        c.wait()
    mine = pl.ds(pl.multiple_of(t * rows, rows), rows)
    own_routes, own_w = l_routes[:, mine], l_weights[:, mine]

    def table(named, first, count):
        slot = lax.broadcasted_iota(jnp.int32, (count * cap, rows), 0)
        index = slot // cap
        place = (slot - index * cap).astype(f32)
        expert = index + first
        hit = jnp.zeros((count * cap, rows), f32)
        for k in range(named.shape[0]):
            hit = jnp.where(named[k : k + 1, :] == expert, 1.0, hit)
        upper = lax.broadcasted_iota(jnp.int32, (rows, rows), 0) < lax.broadcasted_iota(
            jnp.int32, (rows, rows), 1
        )
        earlier = dot(hit.astype(bf16), jnp.where(upper, 1.0, 0.0).astype(bf16))
        return jnp.where(earlier == place, hit, 0.0), expert

    def weighted(chosen, expert, named, given):
        scale = jnp.zeros(chosen.shape, f32)
        for k in range(named.shape[0]):
            scale = jnp.where(named[k : k + 1, :] == expert, given[k : k + 1, :], scale)
        full = jnp.transpose(chosen * scale)
        high = full.astype(bf16)
        return high, (full - high.astype(f32)).astype(bf16)

    chosen, expert = table(own_routes, 0, ep)
    sender = chosen.astype(bf16)

    if levels > 2:
        ready_step(1)
    scales = l_gain[...].astype(f32).reshape(1, width)

    def norm_rows(i, _):
        at = pl.ds(pl.multiple_of(i * 16, 16), 16)
        v = l_tokens[at, :].astype(f32)
        square = jnp.mean(v * v, axis=-1, keepdims=True)
        nf[t, at, :] = (v * lax.rsqrt(square + epsilon) * scales).astype(bf16)
        return 0

    lax.fori_loop(0, rows // 16, norm_rows, 0)

    for k in range(2, levels - 1):
        ready_step(k)

    def table_copies(i):
        return [
            remote(src.at[:, mine], dst.at[i], group_of(to_table + n), gr_recv.at[n], other_gate)
            for n, (src, dst) in enumerate(((l_routes, g_routes), (l_weights, g_weights)))
        ]

    edge = pl.ds(group - 16, 16)
    halos = [
        remote(src.at[edge, :], halo.at[i], group_of(to_halo + i), halo_recv.at[i], (lax.rem(e + 1, ep), t))
        for i, src in enumerate((inner, values))
    ]
    for c in halos:
        c.start()
    if chain:
        for c in table_copies(inner_level):
            c.start()

    def block(i):
        return pl.ds(pl.multiple_of(i * cap, cap), cap)

    def near_dispatch(c, i):
        to = 4 * here + lax.rem(place4 + i, 4)
        at = pl.ds(c * cols, cols)
        return remote(
            og.at[block(to), at], ld.at[block(e), at], group_of(to_gate), d_in.at[c], (to, t)
        )

    def raw_copy(c, i):
        at = pl.ds(c * cols, cols)
        return remote(
            nf.at[t, :, at], g_tokens.at[i, :, at], group_of(to_gate), raw_recv.at[c], other_gate
        )

    def slot_copy(c, i, r):
        at = pl.ds(c * cols, cols)
        return remote(
            g_slots.at[i, block(r), at], ld.at[block(away(i, line)), at],
            group_of(to_slots), d_in.at[c], (4 * here + r, t),
        )

    def forward_slots(c):
        if not chain:
            return
        at = pl.ds(c * cols, cols)

        @pl.when(is_gate)
        def _():
            both = g_slots.at[0, pl.ds(0, 2 * rows), at]
            remote(both, both, group_of(to_gate), raw_recv.at[c], other_gate).wait_recv()
            for i in range(2):
                g_slots[i, :, at] = dot(gate_pick[i], g_tokens[i, :, at]).astype(bf16)
                for r in range(4):

                    @pl.when(place4 != r)
                    def _():
                        slot_copy(c, i, r).start()

                ld[block(away(i, line)), at] = g_slots[i, block(place4), at]

    def dispatch_copy(c, d):
        to = lax.rem(e + d, ep)
        at = pl.ds(c * cols, cols)
        return remote(
            og.at[block(to), at], ld.at[block(e), at], d_send.at[c, d], d_recv.at[c, d], (to, t)
        )

    for c in range(CHUNKS):
        at = pl.ds(c * cols, cols)
        og[:, at] = dot(sender, nf[t, :, at]).astype(bf16)

        if chain:
            raw_copy(c, inner_level).start()
            for i in range(1, 4):
                near_dispatch(c, i).start()
        else:

            def start_dispatch(d, _):
                dispatch_copy(c, d).start()
                return 0

            lax.fori_loop(1, ep, start_dispatch, 0)
        ld[block(e), at] = og[block(e), at]
    if not chain:
        start_x(n_kind)
    for k in range(kinds):
        pair_copy(k).start()
    if chain:
        spread_own()
    else:
        for k in range(3 + NORMED_AT, n_kind):
            start_x(k)


    def pair_sum(j, i):
        return remote(
            parts.at[j, 2 * i + 1 - b], pairs.at[j, i], group_of(to_sums), r_recv.at[j, i], pair
        )

    def far_sum(j, d, c):
        at = pl.ds(c * cols, cols)
        return remote(
            sums.at[j, d - 1, :, at], arrived.at[j, d - 1, :, at],
            group_of(to_sums), rx_recv.at[j, d - 1, c], (e, far(d)),
        )

    def start_far(j):
        for d in range(1, half):
            i = lax.rem(a + d, half)
            pair_sum(j, i).wait_recv()
            for c in range(CHUNKS):
                at = pl.ds(c * cols, cols)
                total = parts[j, 2 * i + b, :, at].astype(f32) + pairs[j, i, :, at].astype(f32)
                sums[j, d - 1, :, at] = total.astype(bf16)
                far_sum(j, d, c).start()

    def own_shared(at):
        return parts[1, t, :, at].astype(f32) + pairs[1, a, :, at].astype(f32)

    def summed(j, c):
        at = pl.ds(c * cols, cols)
        total = parts[j, t, :, at].astype(f32) + pairs[j, a, :, at].astype(f32)
        for d in range(1, half):
            far_sum(j, d, c).wait_recv()
        for d in range(1, half):
            total = total + arrived[j, d - 1, :, at].astype(f32)
        return total

    if chain:
        mix = weighted(chosen, expert, own_routes, own_w)
        wide = 4 * cap
        for h in range(2):
            for n in range(2):
                own_mix[h, n] = mix[n][:, h * wide : (h + 1) * wide]

        @pl.when(is_gate)
        def _():
            for n, ref in enumerate((g_routes, g_weights)):
                remote(ref, ref, group_of(to_table + n), gr_recv.at[n], other_gate).wait_recv()
            for i in range(2):
                named = g_routes[i]
                picked, which = table(named, 4 * here, 4)
                pair_of = weighted(picked, which, named, g_weights[i])
                gate_pick[i] = picked.astype(bf16)
                for n in range(2):
                    gate_mix[i, n] = pair_of[n]

    for c in local[:4]:
        c.wait()
    for c in halos:
        c.wait_recv()
    before = halo[0].astype(f32) * halo[1].astype(f32)
    prod[0:16, :] = jnp.where(e > 0, before, 0.0)
    prod[16:, :] = l_inner[...].astype(f32) * l_values[...].astype(f32)
    tap = l_taps[...].astype(f32)
    for s in range(tp):
        lo = s * rows
        conv = jnp.zeros((rows, ch), f32)
        for j in range(n_taps):
            first = 16 + lo - (n_taps - 1) + j
            conv = conv + tap[j : j + 1, :] * prod[first : first + rows, :]
        gated = (l_outer[lo : lo + rows, :].astype(f32) * conv).astype(bf16)
        for c in range(CHUNKS):
            at = pl.ds(c * cols, cols)
            parts[0, s, :, at] = dot(gated, l_out_w[:, at]).astype(bf16)
        if s == tp // 2 - 1:
            forward_slots(0)
    for i in range(half):
        pair_sum(0, i).start()
    forward_slots(1)

    for c in local[4:]:
        c.wait()

    def shared(s):
        x = nf[s]
        g = dot(x, l_sg[...])
        u = dot(x, l_su[...])
        h = (g / (1.0 + jnp.exp(-g)) * u).astype(bf16)
        for c in range(CHUNKS):
            at = pl.ds(c * cols, cols)
            parts[1, s, :, at] = dot(h, l_sd[:, at]).astype(bf16)

    def shared_hidden(x, gate_w, up_w):
        g = dot(x, gate_w)
        u = dot(x, up_w)
        return (g / (1.0 + jnp.exp(-g)) * u).astype(bf16)

    couple = (t, 2 * a + 1 - b)
    if chain:
        sh_hid[0, 0] = shared_hidden(nf[t], l_sg[...], l_su[...])
        forward_slots(2)
        pair_copy(n_kind).wait_recv()
        sh_hid[0, 1] = shared_hidden(nf[couple[1]], l_sg[...], l_su[...])
        forward_slots(3)
        spread_partner()
        spread_away(True)
    else:
        shared(t)
        pair_copy(n_kind).wait_recv()
        shared(couple[1])
        pair_sum(1, a).start()

    def far_shared():
        wait_pieces()
        for i in (1, 0):
            for d in range(1, half):
                sh_hid[d, i] = shared_hidden(nf[couple[i]], far_g[d - 1], far_u[d - 1])
            for c in range(CHUNKS):
                at = pl.ds(c * cols, cols)
                total = dot(sh_hid[0, i], l_sd[:, at])
                for d in range(1, half):
                    total = total + dot(sh_hid[d, i], far_d[d - 1, :, at])
                parts[1, couple[i], :, at] = total.astype(bf16)
            if i:
                pair_sum(1, a).start()

    def act(s, g, u):
        hid[s] = (g / (1.0 + jnp.exp(-g)) * u).astype(bf16)

    pair_copy(0).wait_recv()
    pair_copy(1).wait_recv()
    close = (t, 2 * a + 1 - b)
    for c in range(CHUNKS):
        at = pl.ds(c * cols, cols)

        if chain:
            for count, mine_too in ((5, is_gate), (7, jnp.logical_not(is_gate))):

                @pl.when(mine_too)
                def _():
                    blocks = ld.at[pl.ds(0, count * cap), at]
                    remote(blocks, blocks, group_of(to_gate), d_in.at[c], pair).wait_recv()

        else:

            def wait_dispatch(d, _):
                dispatch_copy(c, d).wait_recv()
                return 0

            lax.fori_loop(1, ep, wait_dispatch, 0)
        for i, s in enumerate(close):
            g, u = dot(ld[:, at], gf[s, at, :]), dot(ld[:, at], uf[s, at, :])
            if c:
                g, u = g + acc[i, 0], u + acc[i, 1]
            if c < CHUNKS - 1:
                acc[i, 0] = g
                acc[i, 1] = u
            else:
                act(s, g, u)
        if c == 1:
            forward(0)
    wait_forwarded(0)
    rest = [near(d) for d in range(1, half)] + [near(d) + 1 - 2 * b for d in range(1, half)]
    gates = [dot(ld[...], gf[s]) for s in rest]
    forward(1)
    for n, s in enumerate(rest):
        if n == half - 1:
            wait_forwarded(1)
        act(s, gates[n], dot(ld[...], uf[s]))

    def back_copy(c, d):
        to = lax.rem(e + d, ep)
        at = pl.ds(c * bcols, bcols)
        return remote(
            rt.at[block(to), at], rv.at[block(e), at], b_send.at[c, d], b_recv.at[c, d], (to, t)
        )

    def near_copy(c, i):
        to = e + (0, 1 - 2 * line, 2 - 4 * inner_level, 3 - 2 * line - 4 * inner_level)[i]
        at = pl.ds(c * bcols, bcols)
        return remote(
            rt.at[block(to), at], rv.at[block(e), at], group_of(to_back), b_in.at[c], (to, t)
        )

    def gate_of(j):
        return 2 * (1 + here) + j % 2

    def gate_copy(c, j):
        at = pl.ds(c * bcols, bcols)
        return remote(
            rt.at[block(4 - 4 * here + j), at], g_blocks.at[j // 2, block(place4), at],
            group_of(to_back), g_recv.at[c], (gate_of(j), t),
        )

    def row_copy(c, i):
        at = pl.ds(c * bcols, bcols)
        return remote(
            g_rows.at[i, :, at], g_in.at[:, at], group_of(to_rows), b_in.at[c],
            (4 - 4 * here + 2 * i + line, t),
        )

    def start_back(c):
        at = pl.ds(c * bcols, bcols)
        if chain:
            for j in range(4):

                @pl.when(gate_of(j) != e)
                def _():
                    gate_copy(c, j).start()

                @pl.when(gate_of(j) == e)
                def _():
                    g_blocks[j // 2, block(place4), at] = rt[block(4 - 4 * here + j), at]

            for gate, now in ((True, (2,)), (False, (1,))):

                @pl.when(is_gate if gate else jnp.logical_not(is_gate))
                def _():
                    for i in now:
                        near_copy(c, i).start()
                    for m in range(returns if c == returns - 1 else 0):
                        for i in range(1, 4):
                            if i not in now:
                                near_copy(m, i).start()

        else:

            def start_one(d, _):
                back_copy(c, d).start()
                return 0

            lax.fori_loop(1, ep, start_one, 0)
        rv[block(e), at] = rt[block(e), at]

    def wait_back(c):
        if chain:
            got = rt.at[pl.ds(0, 3 * cap + rows), pl.ds(c * bcols, bcols)]
            remote(got, got, group_of(to_back), b_in.at[c], pair).wait_recv()
        else:

            def wait_one(d, _):
                back_copy(c, d).wait_recv()
                return 0

            lax.fori_loop(1, ep, wait_one, 0)

    def merge(c):
        if not chain:
            return
        at = pl.ds(c * bcols, bcols)

        @pl.when(is_gate)
        def _():
            six = rt.at[pl.ds(0, 6 * cap), at]
            remote(six, six, group_of(to_back), g_recv.at[c], pair).wait_recv()
            for i in range(2):
                blocks = g_blocks[i, :, at]
                rows_in = dot(gate_mix[i, 0], blocks) + dot(gate_mix[i, 1], blocks)
                g_rows[i, :, at] = rows_in.astype(bf16)
                row_copy(c, i).start()

    for c in range(returns):
        k = 2 + c
        at = pl.ds(c * bcols, bcols)
        pair_copy(k).wait_recv()
        forward(k)
        wait_forwarded(k)
        total = dot(hid[0], df[0, :, at])
        for s in range(1, tp):
            total = total + dot(hid[s], df[s, :, at])
        rt[:, at] = total.astype(bf16)
        start_back(c)
        if c >= lag:
            merge(c - lag)
        if chain and c == 1:
            start_far(0)
        if chain and c == SPREAD_AT:
            spread_away(False)
        if not chain and c == NORMED_AT:
            start_far(0)
            forward(n_kind)
            for d in range(1, half):
                shared(near(d))
            wait_forwarded(n_kind)
            for d in range(1, half):
                shared(near(d) + 1 - 2 * b)
                pair_sum(1, lax.rem(a + half - d, half)).start()
            start_far(1)
    for c in range(returns - lag, returns):
        merge(c)
    if chain:
        far_shared()

    if not chain:
        mix = weighted(chosen, expert, own_routes, own_w)
    pair_sum(1, a).wait_recv()
    for c in range(returns):
        if c == returns - 1:
            pair_sum(0, a).wait_recv()
            for m in range(CHUNKS):
                at = pl.ds(m * cols, cols)
                mix_o[:, at] = summed(0, m).astype(bf16)
        at = pl.ds(c * bcols, bcols)
        wait_back(c)
        if chain:
            got = rv[pl.ds(pl.multiple_of(here * wide, wide), wide), at]
            routed = dot(own_mix[here, 0], got) + dot(own_mix[here, 1], got)
            routed = routed + g_in[:, at].astype(f32)
        else:
            routed = dot(mix[0], rv[:, at]) + dot(mix[1], rv[:, at])
        exp_o[:, at] = ((own_shared(at) if chain else summed(1, c)) + routed).astype(bf16)


    for c in halos:
        c.wait_send()
    if chain:
        for c in table_copies(inner_level):
            c.wait_send()
        drain(to_gate, og.at[pl.ds(0, 2 * rows + 3 * cap), :])
        drain(to_spread, og.at[pl.ds(0, 9 * unit), :])
        drain(to_x, gf.at[pl.ds(0, 3)])
        drain(to_pair, gf.at[pl.ds(0, 3)])
        drain(to_relay, gf.at[pl.ds(0, 3)])
        drain(to_sums, og.at[pl.ds(0, 4 * rows), :])

        @pl.when(is_gate)
        def _():
            drain(to_slots, og.at[pl.ds(0, 6 * cap), :])
            drain(to_rows, og.at[pl.ds(0, 2 * rows), :])
            drain(to_forward, og.at[pl.ds(0, 6 * unit), :])
            drain(to_back, og.at[pl.ds(0, 5 * cap), :])
            drain(to_pieces, og.at[pl.ds(0, 9 * unit), :])

        @pl.when(jnp.logical_not(is_gate))
        def _():
            drain(to_back, og.at[pl.ds(0, 7 * cap), :])
            drain(to_pieces, og.at[pl.ds(0, 15 * unit), :])

        return

    def sent(d, _):
        for c in range(CHUNKS):
            dispatch_copy(c, d).wait_send()
            back_copy(c, d).wait_send()
        return 0

    lax.fori_loop(1, ep, sent, 0)
    for k in range(kinds):
        pair_copy(k).wait_send()
        for d in range(1, half):
            x_copy(k, d).wait_send()
            forward_copy(k, d).wait_send()
    for j in range(2):
        for i in range(half):
            pair_sum(j, i).wait_send()
        for c in range(CHUNKS):
            for d in range(1, half):
                far_sum(j, d, c).wait_send()


def per_device(
    outer_gate, inner_gate, conv_values, conv_taps, out_weight, moe_input, norm_gain,
    gate_proj, up_proj, down_proj, shared_gate, shared_up, shared_down, routes, route_weight,
):
    tp = lax.axis_size("tp")
    ep = lax.axis_size("ep")
    half = tp // 2
    group, ch = inner_gate.shape
    rows, width = moe_input.shape
    units = gate_proj.shape[2]
    sh_units = shared_gate.shape[1]
    cap = 2 * rows * routes.shape[1] // ep
    cap = -(-cap // 16) * 16
    slots = ep * cap
    returns = RETURNS if ep <= 8 else CHUNKS
    kinds = returns + 3
    vmem = pl.BlockSpec(memory_space=pltpu.VMEM)
    any_spec = pl.BlockSpec(memory_space=pl.ANY)
    dma = pltpu.SemaphoreType.DMA

    direct = (1, 1) if ep <= 8 else (CHUNKS, ep)

    def buf(*shape):
        return pltpu.VMEM(shape, bf16)

    scratch = [
        buf(rows, width), buf(width), buf(*conv_taps.shape),
        pltpu.VMEM((routes.shape[1], group), jnp.int32), pltpu.VMEM((routes.shape[1], group), f32),
        buf(group, ch), buf(group, ch), buf(group, ch), buf(2, 16, ch),
        pltpu.VMEM((group + 16, ch), f32), buf(ch, width),
        buf(width, sh_units), buf(width, sh_units), buf(sh_units, width),
        buf(tp, width, units), buf(tp, width, units), buf(tp, units, width),
        buf(tp, rows, width), buf(slots, width), buf(slots, width),
        buf(tp, slots, units), buf(slots, width), buf(slots, width),
        pltpu.VMEM((2, 2, slots, units), f32), buf(2, tp, rows, width), buf(2, half, rows, width),
        buf(2, half - 1, rows, width), buf(2, half - 1, rows, width),
        dma((15,)), dma((15,)), dma((2,)),
        dma((kinds, 2 * half - 1)), dma(direct), dma(direct), dma(direct), dma(direct),
        dma((2, half)), dma((2, half - 1, CHUNKS)),
        pltpu.SemaphoreType.REGULAR((max(ep // 2 - 1, 1),)),
        pltpu.SemaphoreType.REGULAR((max(ep // 2 - 1, 1),)),
        pltpu.VMEM((2, routes.shape[1], rows), jnp.int32),
        pltpu.VMEM((2, routes.shape[1], rows), f32),
        buf(2, 4 * cap, width), buf(2, rows, width), buf(rows, width),
        buf(2, 2, rows, 4 * cap), buf(2, 2, rows, 4 * cap),
        dma((2,)), dma((returns,)), dma((returns,)),
        buf(2, rows, width), buf(2, 4 * cap, width), buf(2, 4 * cap, rows),
        dma((CHUNKS,)), dma((CHUNKS,)),
        buf(half - 1, width, sh_units), buf(half - 1, width, sh_units), buf(half - 1, sh_units, width),
        buf(half, 2, rows, sh_units),
        dma((3, half - 1)), dma((3, half - 1)), dma((3, half - 1)), dma((half - 1,)), dma((3, half - 1)),
        dma((half - 1,)), dma((3, half - 1)),
    ]
    out = pltpu.VMEM((rows, width), bf16)
    return pl.pallas_call(
        functools.partial(kernel, (ep, tp, cap)),
        out_shape=(out, out),
        in_specs=[any_spec] * 15,
        out_specs=(vmem, vmem),
        scratch_shapes=scratch,
        compiler_params=pltpu.CompilerParams(
            collective_id=0, has_side_effects=True, vmem_limit_bytes=65536000
        ),
    )(
        outer_gate, inner_gate, conv_values, conv_taps, out_weight, moe_input,
        norm_gain, gate_proj, up_proj, down_proj,
        shared_gate, shared_up, shared_down, routes.T, route_weight.T,
    )


def solution(mesh):
    return jax.shard_map(
        per_device,
        mesh=mesh,
        in_specs=(
            P("ep", "tp"), P("ep", "tp"), P("ep", "tp"), P(None, "tp"), P("tp", None),
            P(("ep", "tp"), None), P(),
            P("ep", None, "tp"), P("ep", None, "tp"), P("ep", "tp", None),
            P(None, "tp"), P(None, "tp"), P("tp", None), P("ep", None), P("ep", None),
        ),
        out_specs=(P(("ep", "tp"), None), P(("ep", "tp"), None)),
        check_vma=False,
    )
```
